512 devices in a mesh: sp: 32 (over z, x), tp: 16 (over y, core).
Axes of the slice: x: 4, y: 8, z: 8, core: 2. Of those that a mesh axis runs over, the one named last changes fastest.
Arguments:
- glu_value: bfloat16 [1024, 8192], P('tp', 'sp')
- glu_gate: bfloat16 [1024, 8192], P('tp', 'sp'), may hold values from -8 to 8
- conv_taps: float32 [1024, 31], P('tp'), may hold values from -1 to 1
- norm_gain: float32 [1024], P('tp'), may hold values from 0.1 to 1.9
- out_proj: bfloat16 [1024, 2048], P(None, 'tp'), may hold values from -0.1875 to 0.1875
- resid: bfloat16 [8192, 2048], P('sp', 'tp'), may hold values from -6 to 6
- expert_ids: int32 [8192, 2], P('sp'), may hold values from 0 to 31, all different within a row; in each aligned block of 256 rows (0 to 255, 256 to 511, ...) at most 32 rows name the same one
- route_logits: float32 [8192, 2], P('sp'), may hold values from -8 to 8
- group_prob: float32 [8192], P('sp'), may hold values from 0.2 to 1
- w_gate: bfloat16 [32, 2048, 4096], P('sp', None, 'tp'), may hold values from -0.125 to 0.125
- w_up: bfloat16 [32, 2048, 4096], P('sp', None, 'tp'), may hold values from -0.125 to 0.125
- w_down: bfloat16 [32, 4096, 2048], P('sp', None, 'tp'), may hold values from -0.09375 to 0.09375
Outputs:
- layer_out: bfloat16 [8192, 2048], P('sp', 'tp')
The draws below stay inside these ranges and needn't reach their ends.
Inputs may be any that keep to these rules, and one draw needn't show every extreme that they name: `expert_ids`: each row names 2 different experts. In each aligned block of 256 rows (the rows of one index of sp) no expert is named by more than 32 rows, a bound that some block reaches.
All inputs are finite; a program needn't handle non-finite values.
Results may differ from the reference program's by a relative error of at most 0.0061.
Values may be sent and summed in bfloat16 or wider, within the bound.
A program may use at most 64 MiB of HBM per device.

```python
import math
import jax
import jax.numpy as jnp
import numpy as np
from jax import lax

D = 2048
CH = 1024
FF = 4096
KW = 31
TOPK = 2
TOK_DEV = 256
TOKENS = 8192
EXPERTS = 32
CAP = 32
N_SP = 32


def draw_glu_value(key, part):
    keyset = jax.random.split(key, 2)
    position = jnp.arange(CH, dtype=jnp.float32) / CH
    column = 10.0 ** position * jax.random.uniform(keyset[1], (CH,), jnp.float32, 0.5, 1.5)
    sample = jax.random.normal(keyset[0], (CH, TOKENS), jnp.float32)
    return (sample * column[:, None]).astype(jnp.bfloat16)


def block_scale(own_key, extent, cuts, smallest, largest):
    loudness = 1.0
    for axis_at, parts in cuts:
        steps = jax.random.uniform(jax.random.fold_in(jax.random.fold_in(own_key, 6), axis_at), (parts,), jnp.float32, smallest / len(cuts), largest / len(cuts))
        loudness = loudness * jnp.repeat(jnp.exp(steps), extent[axis_at] // parts).reshape((-1,) + (1,) * (len(extent) - 1 - axis_at))
    return loudness


def routed_block(rng, own, number, rows, amount, top, bound, slope):
    order = jax.random.permutation(rng, amount)
    packed, usual = shares(amount, rows * top, bound, slope, True), shares(amount, rows * top, bound, slope, False)
    places = jnp.arange(amount)

    def named(sizes, rotation):
        used = int((sizes > 0).sum())
        fixed = max(1, used // 4)
        passed = fixed + (places - fixed + rotation * (used - fixed)) % max(1, amount - fixed)
        return jnp.zeros((amount,), jnp.int32).at[order[jnp.where(places < fixed, places, passed)]].set(jnp.asarray(sizes, jnp.int32))

    sizes = jnp.where(number % 4 == 0, named(packed, number // 4), named(usual, number - number // 4 - 1))
    mixed = jax.random.permutation(jax.random.fold_in(own, 3), amount)
    donor, sink = mixed[0:amount // 2 * 2:2], mixed[1:amount // 2 * 2:2]
    margin = jnp.minimum(sizes[donor] - 1, bound - sizes[sink]) // 2
    margin = jnp.where((donor == order[0]) | (sink == order[0]) | (sizes[sink] == 0), 0, jnp.maximum(margin, 0))
    passed = jax.random.randint(jax.random.fold_in(own, 4), (amount // 2,), 0, 1 << 20) % (margin + 1)
    sizes = sizes.at[donor].add(-passed).at[sink].add(passed)
    members = jnp.searchsorted(jnp.cumsum(sizes), jnp.arange(rows * top), side="right").astype(jnp.int32)
    listing = members.reshape(top, rows).T
    listing = listing[jax.random.permutation(jax.random.fold_in(own, 1), rows)]
    rotation = jax.random.randint(jax.random.fold_in(own, 2), (rows, 1), 0, top)
    return jnp.take_along_axis(listing, (jnp.arange(top)[None, :] + rotation) % top, axis=1)


def shares(count, total, reach, slope, full):
    portions = [(1 << 20) // math.isqrt(rank ** slope) + 1 for rank in range(1, count + 1)]
    largest = reach if full else min(reach, max(-(-total // count), total * portions[0] // sum(portions)))
    least = 1 if total - largest >= count - 1 else 0
    holding, surplus = [largest] + [least] * (count - 1), total - largest - least * (count - 1)
    while surplus > 0:
        free = [i for i in range(1, count) if holding[i] < largest] or [i for i in range(1, count) if holding[i] < reach]
        pool, left = sum([portions[i] for i in free]), surplus
        for i in free:
            more = min(reach - holding[i], max(1, left * portions[i] // pool), surplus)
            holding[i] = holding[i] + more
            surplus = surplus - more
    return np.array(holding)


def scatter_about(rng, dims, scale, most, shards=(), kind=jnp.bfloat16):
    entries = scale * jax.random.normal(rng, dims, jnp.float32)
    if shards:
        entries = entries * block_scale(rng, dims, shards, -0.22, 0.18)
    return jnp.clip(entries, -most, most).astype(kind)


def setup_inputs(seed: int = 0) -> dict:
    key_list = jax.random.split(jax.random.key(seed), 13)
    glu_value = draw_glu_value(jax.random.fold_in(key_list[12], 71), 0)
    glu_gate = scatter_about(key_list[1], (CH, TOKENS), 1.5, 8.0, ((0, 16), (1, 32)))
    conv_taps = scatter_about(key_list[2], (CH, KW), KW ** -0.5, 1.0, ((0, 16),), jnp.float32)
    norm_gain = jnp.clip(1.0 + 0.18 * jax.random.normal(key_list[3], (CH,), jnp.float32), 0.1, 1.9)
    out_proj = scatter_about(key_list[4], (CH, D), CH ** -0.5, 0.1875, ((1, 16),))
    resid = scatter_about(key_list[5], (TOKENS, D), 1.0, 6.0, ((0, 32), (1, 16)))
    expert_ids_keys = jax.random.split(jax.random.fold_in(key_list[6], 1), TOKENS // TOK_DEV)
    expert_ids_turns = jax.random.permutation(jax.random.fold_in(key_list[6], 3), TOKENS // TOK_DEV)
    expert_ids = jax.vmap(lambda own, number: routed_block(jax.random.fold_in(key_list[6], 2), own, number, TOK_DEV, EXPERTS, TOPK, CAP, 2))(expert_ids_keys, expert_ids_turns).reshape((TOKENS, TOPK))
    route_logits = scatter_about(key_list[7], (TOKENS, TOPK), 1.5, 8.0, ((0, 32),), jnp.float32)
    group_prob = jnp.clip(jnp.exp(math.log(1.0) - 1.609438 * jax.random.uniform(key_list[8], (TOKENS,), jnp.float32) ** block_scale(key_list[8], (TOKENS,), ((0, 32),), -0.2, 0.2)), 0.2, 1.0)
    w_gate = scatter_about(key_list[9], (EXPERTS, D, FF), D ** -0.5, 0.125, ((0, 32), (2, 16)))
    w_up = scatter_about(key_list[10], (EXPERTS, D, FF), D ** -0.5, 0.125, ((0, 32), (2, 16)))
    w_down = scatter_about(key_list[11], (EXPERTS, FF, D), FF ** -0.5, 0.09375, ((0, 32), (2, 16)))
    return dict(glu_value=glu_value, glu_gate=glu_gate, conv_taps=conv_taps, norm_gain=norm_gain, out_proj=out_proj, resid=resid, expert_ids=expert_ids, route_logits=route_logits, group_prob=group_prob, w_gate=w_gate, w_up=w_up, w_down=w_down)


def reference(glu_value, glu_gate, conv_taps, norm_gain, out_proj, resid, expert_ids, route_logits, group_prob, w_gate, w_up, w_down):
    gated = (glu_value.astype(jnp.float32) * jax.nn.sigmoid(glu_gate.astype(jnp.float32))).astype(jnp.bfloat16)
    padded = jnp.pad(gated.astype(jnp.float32), ((0, 0), (KW - 1, 0)))
    filtered = jnp.zeros((CH, TOKENS), jnp.float32)
    for offset in range(KW):
        filtered = filtered + conv_taps[:, offset:offset + 1] * padded[:, offset:offset + TOKENS]
    mean = lax.optimization_barrier(jnp.sum(filtered, axis=0)) / CH
    meansq = lax.optimization_barrier(jnp.sum(filtered * filtered, axis=0)) / CH
    var = meansq - mean * mean
    normed = (filtered - mean[None, :]) * lax.rsqrt(var[None, :] + 1e-05) * norm_gain[:, None]
    activated = jax.nn.silu(normed).astype(jnp.bfloat16)
    projected = lax.dot_general(activated, out_proj, (((0,), (0,)), ((), ())), preferred_element_type=jnp.float32)
    mixed = (resid.astype(jnp.float32) + projected).astype(jnp.bfloat16)
    route_weight = group_prob[:, None] * jax.nn.softmax(route_logits, axis=-1)
    most_rows = N_SP * CAP

    def one_expert(carry, inputs):
        index, gate_mat, up_mat, down_mat = inputs
        chosen = expert_ids == index
        named = jnp.any(chosen, axis=1)
        row_index = jnp.nonzero(named, size=most_rows, fill_value=0)[0].astype(jnp.int32)
        valid = jnp.arange(most_rows) < jnp.sum(named.astype(jnp.int32))
        weight_row = lax.optimization_barrier(jnp.sum(jnp.where(chosen, route_weight, 0.0), axis=1))
        rows = jnp.take(mixed, row_index, axis=0)
        gate_part = jnp.dot(rows, gate_mat, preferred_element_type=jnp.float32)
        up_part = jnp.dot(rows, up_mat, preferred_element_type=jnp.float32)
        hidden = (jax.nn.silu(gate_part) * up_part).astype(jnp.bfloat16)
        expert_out = jnp.dot(hidden, down_mat, preferred_element_type=jnp.float32).astype(jnp.bfloat16)
        scaled = jnp.where(valid, jnp.take(weight_row, row_index), 0.0)
        carry = carry.at[row_index].add(scaled[:, None] * expert_out.astype(jnp.float32))
        return (carry, None)
    routed, _ = lax.scan(one_expert, jnp.zeros((TOKENS, D), jnp.float32), (jnp.arange(EXPERTS, dtype=jnp.int32), w_gate, w_up, w_down))
    return (mixed.astype(jnp.float32) + routed).astype(jnp.bfloat16)
```

```python
import functools
import jax
import jax.numpy as jnp
from jax import lax
from jax.experimental import pallas as pl
from jax.experimental.pallas import tpu as pltpu
from jax.sharding import PartitionSpec as P

BF = jnp.bfloat16
F32 = jnp.float32
MESH = pl.DeviceIdType.MESH


def from_behind(block, axis, distance):
    devices = range(lax.axis_size(axis))
    route = [(i - distance, i) for i in devices if i - distance in devices]
    return lax.ppermute(block, axis, route)


def from_everyone(shard, axis):
    copies = jnp.broadcast_to(shard, (lax.axis_size(axis), *shard.shape))
    return lax.all_to_all(copies, axis, split_axis=0, concat_axis=0, tiled=True)


def of_everyone(shard, axis):
    everything = from_everyone(shard, axis)
    return jnp.sum(everything, axis=0)


def packed_total(arrays, axis):
    ends = [0]
    for a in arrays:
        ends.append(ends[-1] + a.size)
    subtotal = of_everyone(jnp.concatenate([a.ravel() for a in arrays]), axis)
    return tuple((subtotal[b:e].reshape(a.shape) for a, b, e in zip(arrays, ends, ends[1:])))


def dot(a, b):
    return jnp.dot(a, b, preferred_element_type=F32)


def moe_kernel(
    dims,
    mixed_ref,
    ids_ref,
    idst_ref,
    logits_ref,
    prob_ref,
    wg_hbm,
    wu_hbm,
    wd_hbm,
    out_ref,
    wg,
    wu,
    wd,
    outg,
    rows,
    hid,
    res,
    ret,
    wsem,
    dsend,
    drecv,
    rring,
    rsib,
    rsend,
    hring,
    hsib,
    hsend,
    bsend,
    brecv,
):
    nx, nz, ny, cap = dims
    experts = nx * nz
    chunk = nx * cap
    ha = ny // 2
    hb = ny - 1 - ha
    tokens, width = mixed_ref.shape
    ffw = wg.shape[1]
    s = lax.axis_index("sp")
    j = lax.axis_index("tp")
    z, x = s // nx, s % nx
    y, c = j // 2, j % 2
    sib = 2 * y + (1 - c)

    barrier = pltpu.get_barrier_semaphore()

    def greet(k, carry):
        pl.semaphore_signal(barrier, inc=1, device_id=((s + k) % experts, j), device_id_type=MESH)
        return carry

    lax.fori_loop(1, experts, greet, 0)
    for tgt in (2 * ((y + 1) % ny) + c, 2 * ((y + ny - 1) % ny) + c, sib):
        pl.semaphore_signal(barrier, inc=1, device_id=(s, tgt), device_id_type=MESH)

    loads = [
        pltpu.make_async_copy(a.at[0], b, wsem.at[n])
        for n, (a, b) in enumerate(((wg_hbm, wg), (wu_hbm, wu), (wd_hbm, wd)))
    ]
    for load in loads:
        load.start()

    def offset(i):
        return ((i + 1) // 2) * (1 - 2 * ((i + 1) % 2))

    id0 = idst_ref[0:1, :]
    id1 = idst_ref[1:2, :]
    e_io = lax.broadcasted_iota(jnp.int32, (experts, tokens), 0)
    named = jnp.where((e_io == id0) | (e_io == id1), 1.0, 0.0)
    r_io = lax.broadcasted_iota(jnp.int32, (tokens, tokens), 0)
    c_io = lax.broadcasted_iota(jnp.int32, (tokens, tokens), 1)
    upper = jnp.where(r_io < c_io, 1.0, 0.0).astype(BF)
    before = dot(named.astype(BF), upper)
    slot0 = jnp.sum(jnp.where(e_io == id0, before, 0.0), axis=0, keepdims=True) + id0.astype(F32) * cap
    slot1 = jnp.sum(jnp.where(e_io == id1, before, 0.0), axis=0, keepdims=True) + id1.astype(F32) * cap
    s_io = lax.broadcasted_iota(jnp.int32, (experts * cap, tokens), 0).astype(F32)
    pick = jnp.where((s_io == slot0) | (s_io == slot1), 1.0, 0.0).astype(BF)
    outg[...] = dot(pick, mixed_ref[...]).astype(BF)
    own_col = pl.ds(pl.multiple_of(j * width, width), width)
    own_row = pl.ds(pl.multiple_of(x * cap, cap), cap)
    rows[z, own_row, own_col] = outg[pl.ds(pl.multiple_of(s * cap, cap), cap), :]

    pl.semaphore_wait(barrier, experts - 1 + 3)

    def dispatch(n, carry):
        i, dx = n // nx, n % nx
        zt = (z - offset(i) + nz) % nz
        xt = (x + dx) % nx
        e = zt * nx + xt
        pltpu.make_async_remote_copy(
            src_ref=outg.at[pl.ds(pl.multiple_of(e * cap, cap), cap), :],
            dst_ref=rows.at[z, own_row, own_col],
            send_sem=dsend,
            recv_sem=drecv.at[z],
            device_id=(e, j),
            device_id_type=MESH,
        ).start()
        return carry

    lax.fori_loop(1, experts, dispatch, 0)

    def block(buf, wide, q, origin):
        return buf.at[q, :, pl.ds(pl.multiple_of(origin * wide, wide), wide)]

    def push(buf, wide, q, i, origin_y, hop, leg, ring, send, sgn):
        ref = block(buf, wide, q, 2 * origin_y + c)
        step = sgn * (1 - 2 * leg)
        pltpu.make_async_remote_copy(
            src_ref=ref,
            dst_ref=ref,
            send_sem=send.at[i],
            recv_sem=ring.at[i, leg * ha + hop],
            device_id=(s, 2 * ((y + step + ny) % ny) + c),
            device_id_type=MESH,
        ).start()

    def share(buf, wide, q, i, origin_y, sem, send):
        ref = block(buf, wide, q, 2 * origin_y + c)
        pltpu.make_async_remote_copy(
            src_ref=ref,
            dst_ref=ref,
            send_sem=send.at[i],
            recv_sem=sem.at[i],
            device_id=(s, sib),
            device_id_type=MESH,
        ).start()

    def arrived(ref, sem):
        pltpu.make_async_copy(ref, ref, sem).wait()

    def open_ring(buf, wide, q, i, ring, sibs, send):
        sgn = 1 - 2 * (i % 2)
        push(buf, wide, q, i, y, 0, 0, ring, send, sgn)
        if hb > 0:
            push(buf, wide, q, i, y, 0, 1, ring, send, sgn)
        share(buf, wide, q, i, y, sibs, send)

    def hop_ring(h, buf, wide, q, i, ring, sibs, send):
        sgn = 1 - 2 * (i % 2)
        for leg, reach in ((0, ha), (1, hb)):
            if h > reach:
                continue
            origin = (y - sgn * (1 - 2 * leg) * h + 2 * ny) % ny
            arrived(block(buf, wide, q, 2 * origin + c), ring.at[i, leg * ha + h - 1])
            if h < reach:
                push(buf, wide, q, i, origin, h, leg, ring, send, sgn)
            share(buf, wide, q, i, origin, sibs, send)

    def tick(t, carry):
        def at(stage, body):
            i = t - stage

            @pl.when((i >= 0) & (i < nz))
            def _():
                body(i, (z + offset(i) + nz) % nz)

        def rows_open(i, q):
            @pl.when(i == 0)
            def _():
                if nx > 1:
                    arrived(outg.at[pl.ds(0, (nx - 1) * cap), :], drecv.at[q])

            @pl.when(i > 0)
            def _():
                arrived(outg.at[pl.ds(0, nx * cap), :], drecv.at[q])

            open_ring(rows, width, q, i, rring, rsib, rsend)

        def rows_hop(h, i, q):
            hop_ring(h, rows, width, q, i, rring, rsib, rsend)

        def hid_hop(h, i, q):
            hop_ring(h, hid, ffw, q, i, hring, hsib, hsend)

        def first(i, q):
            @pl.when(i == 0)
            def _():
                loads[0].wait()
                loads[1].wait()

            arrived(rows.at[q, :, pl.ds(0, ny * width)], rsib.at[i])
            r = rows[q]
            g = dot(r, wg[...])
            u = dot(r, wu[...])
            h = (g / (1.0 + jnp.exp(-g))) * u
            hid[q, :, pl.ds(pl.multiple_of(j * ffw, ffw), ffw)] = h.astype(BF)
            open_ring(hid, ffw, q, i, hring, hsib, hsend)

        def second(i, q):
            @pl.when(i == 0)
            def _():
                loads[2].wait()

            arrived(hid.at[q, :, pl.ds(0, ny * ffw)], hsib.at[i])
            res[i] = dot(hid[q], wd[...]).astype(BF)
            for xt in range(nx):
                tgt = q * nx + xt
                dst = ret.at[pl.ds(pl.multiple_of(s * cap, cap), cap), :]

                @pl.when(tgt == s)
                def _():
                    ret[pl.ds(pl.multiple_of(s * cap, cap), cap), :] = res[i, pl.ds(xt * cap, cap), :]

                @pl.when(tgt != s)
                def _():
                    pltpu.make_async_remote_copy(
                        src_ref=res.at[i, pl.ds(xt * cap, cap), :],
                        dst_ref=dst,
                        send_sem=bsend,
                        recv_sem=brecv,
                        device_id=(tgt, j),
                        device_id_type=MESH,
                    ).start()

        at(0, rows_open)
        for h in range(1, ha + 1):
            at(h, functools.partial(rows_hop, h))
        for h in range(1, ha + 1):
            at(ha + 1 + h, functools.partial(hid_hop, h))
        at(2 * ha + 2, second)
        at(ha + 1, first)
        return carry

    lax.fori_loop(0, nz + 2 * ha + 2, tick, 0)

    id0 = ids_ref[:, 0:1]
    id1 = ids_ref[:, 1:2]
    e_io = lax.broadcasted_iota(jnp.int32, (tokens, experts), 1)
    named = jnp.where((e_io == id0) | (e_io == id1), 1.0, 0.0)
    lower = jnp.where(c_io < r_io, 1.0, 0.0).astype(BF)
    before = dot(lower, named.astype(BF))
    slot0 = jnp.sum(jnp.where(e_io == id0, before, 0.0), axis=1, keepdims=True) + id0.astype(F32) * cap
    slot1 = jnp.sum(jnp.where(e_io == id1, before, 0.0), axis=1, keepdims=True) + id1.astype(F32) * cap
    s_io = lax.broadcasted_iota(jnp.int32, (tokens, experts * cap), 1).astype(F32)
    pick0 = jnp.where(s_io == slot0, 1.0, 0.0).astype(BF)
    pick1 = jnp.where(s_io == slot1, 1.0, 0.0).astype(BF)
    l0 = logits_ref[:, 0:1]
    l1 = logits_ref[:, 1:2]
    top = jnp.maximum(l0, l1)
    e0 = jnp.exp(l0 - top)
    e1 = jnp.exp(l1 - top)
    scale = prob_ref[...] / (e0 + e1)
    far = outg.at[pl.ds(0, (experts - 1) * cap), :]
    arrived(far, brecv)
    back = ret[...]
    routed = dot(pick0, back) * (e0 * scale) + dot(pick1, back) * (e1 * scale)
    out_ref[...] = (mixed_ref[...].astype(F32) + routed).astype(BF)

    arrived(far, dsend)
    arrived(far, bsend)

    def drain(i, carry):
        arrived(rows.at[0, :, pl.ds(0, (2 * ny - 1) * width)], rsend.at[i])
        arrived(hid.at[0, :, pl.ds(0, (2 * ny - 1) * ffw)], hsend.at[i])
        return carry

    lax.fori_loop(0, nz, drain, 0)


def moe(mixed, ids, logits, prob, w_gate, w_up, w_down):
    sp, tp = lax.axis_size("sp"), lax.axis_size("tp")
    nx = 4 if sp % 8 == 0 else 1
    nz, ny = sp // nx, tp // 2
    tokens, width = mixed.shape
    cap = 4 * tokens // sp
    depth, ffw = w_gate.shape[1:]
    chunk = nx * cap
    ha = ny // 2
    dma = pltpu.SemaphoreType.DMA
    vmem = pl.BlockSpec(memory_space=pltpu.VMEM)
    hbm = pl.BlockSpec(memory_space=pl.ANY)
    return pl.pallas_call(
        functools.partial(moe_kernel, (nx, nz, ny, cap)),
        out_shape=jax.ShapeDtypeStruct((tokens, width), BF),
        in_specs=[vmem] * 5 + [hbm] * 3,
        out_specs=vmem,
        scratch_shapes=[
            pltpu.VMEM((depth, ffw), BF),
            pltpu.VMEM((depth, ffw), BF),
            pltpu.VMEM(w_down.shape[1:], BF),
            pltpu.VMEM((sp * cap, width), BF),
            pltpu.VMEM((nz, chunk, depth), BF),
            pltpu.VMEM((nz, chunk, tp * ffw), BF),
            pltpu.VMEM((nz, chunk, width), BF),
            pltpu.VMEM((sp * cap, width), BF),
            dma((3,)),
            dma(()),
            dma((nz,)),
            dma((nz, ny - 1)),
            dma((nz,)),
            dma((nz,)),
            dma((nz, ny - 1)),
            dma((nz,)),
            dma((nz,)),
            dma(()),
            dma(()),
        ],
        compiler_params=pltpu.CompilerParams(
            collective_id=0, has_side_effects=True, vmem_limit_bytes=40 * 1024 * 1024
        ),
    )(mixed, ids, ids.T, logits, prob[:, None], w_gate, w_up, w_down)


def per_device(
    glu_value,
    glu_gate,
    conv_taps,
    norm_gain,
    out_proj,
    resid,
    expert_ids,
    route_logits,
    group_prob,
    w_gate,
    w_up,
    w_down,
):
    local_tokens = glu_value.shape[1]
    tap_count = conv_taps.shape[1]
    channels = glu_value.shape[0] * lax.axis_size("tp")
    gated = (glu_value.astype(F32) * jax.nn.sigmoid(glu_gate.astype(F32))).astype(BF)
    history = from_behind(gated[:, local_tokens - (tap_count - 1) :], "sp", 1)
    padded = jnp.concatenate([history, gated], axis=1).astype(F32)
    filtered = jnp.zeros(gated.shape, F32)
    for offset in range(tap_count):
        filtered = (
            filtered + conv_taps[:, offset : offset + 1] * padded[:, offset : offset + local_tokens]
        )
    total_one, total_two = packed_total(
        (jnp.sum(filtered, axis=0), jnp.sum(filtered * filtered, axis=0)), "tp"
    )
    mean = total_one / channels
    var = total_two / channels - mean * mean
    normed = (filtered - mean[None, :]) * lax.rsqrt(var[None, :] + 1e-05) * norm_gain[:, None]
    activated = jax.nn.silu(normed).astype(BF)
    projected = lax.dot_general(
        lax.all_gather(activated, "tp", axis=0, tiled=True),
        out_proj,
        (((0,), (0,)), ((), ())),
        preferred_element_type=F32,
    )
    mixed = (resid.astype(F32) + projected).astype(BF)
    return moe(mixed, expert_ids, route_logits, group_prob, w_gate, w_up, w_down)


def solution(mesh):
    return jax.shard_map(
        per_device,
        mesh=mesh,
        in_specs=(
            P("tp", "sp"),
            P("tp", "sp"),
            P("tp", None),
            P("tp"),
            P(None, "tp"),
            P("sp", "tp"),
            P("sp", None),
            P("sp", None),
            P("sp"),
            P("sp", None, "tp"),
            P("sp", None, "tp"),
            P("sp", None, "tp"),
        ),
        out_specs=P("sp", "tp"),
        check_vma=False,
    )
```

```python
import functools
import jax
import jax.numpy as jnp
from jax import lax
from jax.experimental import pallas as pl
from jax.experimental.pallas import tpu as pltpu
from jax.sharding import PartitionSpec as P

BF = jnp.bfloat16
F32 = jnp.float32
MESH = pl.DeviceIdType.MESH
LANES = 128


def dot(a, b):
    return jnp.dot(a, b, preferred_element_type=F32)


def layer_kernel(
    dims,
    gv_hbm,
    gg_hbm,
    taps_ref,
    gain_ref,
    proj_hbm,
    resid_hbm,
    ids_ref,
    logits_ref,
    prob_ref,
    wg_hbm,
    wu_hbm,
    wd_hbm,
    out_ref,
    gv,
    gg,
    proj,
    resid,
    wg,
    wu,
    wd,
    wdt,
    tapcol,
    tail,
    halo,
    stats,
    act,
    pick,
    pick0,
    pick1,
    scales,
    mixed,
    outg,
    rows,
    own,
    give,
    take,
    sumout,
    sumin,
    res,
    ret,
    lsem,
    halo_s,
    halo_r,
    stat_s,
    stat_r,
    act_s,
    act_r,
    act_sib,
    wdt_s,
    wdt_r,
    dsend,
    drecv,
    rring,
    rsib,
    rsend,
    sib_s,
    sib_r,
    sum_s,
    sum_r,
    bsend,
    brecv,
):
    nx, nz, ny, cap, taps, channels = dims
    experts = nx * nz
    chunk = nx * cap
    tp = 2 * ny
    ha = ny // 2
    hb = ny - 1 - ha
    tokens, width = out_ref.shape
    own_ch = gv.shape[0]
    ffw = wg.shape[1]
    s = lax.axis_index("sp")
    j = lax.axis_index("tp")
    z, x = s // nx, s % nx
    y, c = j // 2, j % 2
    sib = 2 * y + (1 - c)

    def remote(src, dst, send, recv, where):
        pltpu.make_async_remote_copy(
            src_ref=src,
            dst_ref=dst,
            send_sem=send,
            recv_sem=recv,
            device_id=where,
            device_id_type=MESH,
        ).start()

    def arrived(ref, sem):
        pltpu.make_async_copy(ref, ref, sem).wait()

    def rows_of(n, size):
        return pl.ds(pl.multiple_of(n * size, size), size)

    loads = [
        pltpu.make_async_copy(a, b, lsem.at[n])
        for n, (a, b) in enumerate(
            (
                (gv_hbm, gv),
                (gg_hbm, gg),
                (wd_hbm.at[0], wd),
                (proj_hbm, proj),
                (resid_hbm, resid),
                (wg_hbm.at[0], wg),
                (wu_hbm.at[0], wu),
            )
        )
    ]
    for load in loads:
        load.start()

    barrier = pltpu.get_barrier_semaphore()

    def greet_sp(k, carry):
        pl.semaphore_signal(barrier, inc=1, device_id=((s + k) % experts, j), device_id_type=MESH)
        return carry

    def greet_tp(k, carry):
        pl.semaphore_signal(barrier, inc=1, device_id=(s, (j + k) % tp), device_id_type=MESH)
        return carry

    lax.fori_loop(1, experts, greet_sp, 0)
    lax.fori_loop(1, tp, greet_tp, 0)

    loads[0].wait()
    loads[1].wait()
    gated = (gv[...].astype(F32) * jax.nn.sigmoid(gg[...].astype(F32))).astype(BF)
    tail[...] = gated[:, tokens - LANES :]

    id0 = ids_ref[0:1, :]
    id1 = ids_ref[1:2, :]
    e_io = lax.broadcasted_iota(jnp.int32, (experts, tokens), 0)
    named = jnp.where((e_io == id0) | (e_io == id1), 1.0, 0.0)
    r_io = lax.broadcasted_iota(jnp.int32, (tokens, tokens), 0)
    c_io = lax.broadcasted_iota(jnp.int32, (tokens, tokens), 1)
    upper = jnp.where(r_io < c_io, 1.0, 0.0).astype(BF)
    before = dot(named.astype(BF), upper)
    slot0 = jnp.sum(jnp.where(e_io == id0, before, 0.0), axis=0, keepdims=True) + id0.astype(F32) * cap
    slot1 = jnp.sum(jnp.where(e_io == id1, before, 0.0), axis=0, keepdims=True) + id1.astype(F32) * cap
    s_io = lax.broadcasted_iota(jnp.int32, (experts * cap, tokens), 0).astype(F32)
    pick[...] = jnp.where((s_io == slot0) | (s_io == slot1), 1.0, 0.0).astype(BF)
    l0 = logits_ref[0:1, :]
    l1 = logits_ref[1:2, :]
    top = jnp.maximum(l0, l1)
    e0 = jnp.exp(l0 - top)
    e1 = jnp.exp(l1 - top)
    scale = prob_ref[...] / (e0 + e1)
    k_io = lax.broadcasted_iota(jnp.int32, (8, tokens), 0)
    stack = jnp.where(
        k_io == 0, slot0, jnp.where(k_io == 1, slot1, jnp.where(k_io == 2, e0 * scale, e1 * scale))
    )
    cols = stack.T
    scales[...] = cols
    t_io = lax.broadcasted_iota(jnp.int32, (tokens, experts * cap), 1).astype(F32)
    pick0[...] = jnp.where(t_io == cols[:, 0:1], 1.0, 0.0).astype(BF)
    pick1[...] = jnp.where(t_io == cols[:, 1:2], 1.0, 0.0).astype(BF)
    tapcol[...] = jnp.zeros_like(tapcol)
    tapcol[0:taps, 0:own_ch] = taps_ref[...]
    tapcol[taps : taps + 1, 0:own_ch] = gain_ref[...]
    tap = tapcol[...].T

    loads[2].wait()
    wdt[j] = wd[rows_of(j, ffw), :]

    pl.semaphore_wait(barrier, experts - 1 + tp - 1)

    def give_wd(peer_y, peer_c):
        peer = 2 * peer_y + peer_c
        remote(wd.at[rows_of(peer, ffw), :], wdt.at[j], wdt_s, wdt_r, (s, peer))

    def give_wd_at(reach):
        for d in sorted({reach % ny, (ny - reach) % ny}):
            give_wd((y + d) % ny, c)
            give_wd((y + d) % ny, 1 - c)

    @pl.when(s < experts - 1)
    def _():
        remote(tail, halo, halo_s, halo_r, ((s + 1) % experts, j))

    give_wd(y, 1 - c)
    give_wd_at(1)

    @pl.when(s == 0)
    def _():
        halo[...] = jnp.zeros_like(halo)

    @pl.when(s > 0)
    def _():
        arrived(halo, halo_r)

    padded = jnp.concatenate([halo[...], gated], axis=1).astype(F32)
    filtered = jnp.zeros((own_ch, tokens), F32)
    for o in range(taps):
        shift = taps - 1 - o
        moved = pltpu.roll(padded, shift, 1) if shift else padded
        filtered = filtered + tap[0:own_ch, o : o + 1] * moved[:, LANES:]
    stats[j, 0:1, :] = jnp.sum(filtered, axis=0, keepdims=True)
    stats[j, 1:2, :] = jnp.sum(filtered * filtered, axis=0, keepdims=True)

    def give_stats(k, carry):
        remote(stats.at[j], stats.at[j], stat_s, stat_r, (s, (j + k) % tp))
        return carry

    lax.fori_loop(1, tp, give_stats, 0)
    if ny > 2:
        give_wd_at(2)
    arrived(stats.at[pl.ds(0, tp - 1)], stat_r)
    totals = jnp.sum(stats[...], axis=0)
    mean = totals[0:1] / channels
    var = totals[1:2] / channels - mean * mean
    normed = (filtered - mean) * lax.rsqrt(var + 1e-05) * tap[0:own_ch, taps : taps + 1]
    act[j] = (normed / (1.0 + jnp.exp(-normed))).astype(BF)

    near = []
    for d in range(1, ha + 1):
        near.append(d)
        if ny - d != d:
            near.append(ny - d)
    for d in near:
        remote(act.at[j], act.at[j], act_s, act_r.at[d], (s, 2 * ((y + d) % ny) + c))
    remote(act.at[j], act.at[j], act_s, act_sib, (s, sib))
    for reach in range(3, ha + 1):
        give_wd_at(reach)
    for d in near:
        k = 2 * ((y + ny - d) % ny) + c
        arrived(act.at[k], act_r.at[d])
        remote(act.at[k], act.at[k], act_s, act_sib, (s, sib))
    arrived(act.at[pl.ds(0, ny)], act_sib)
    loads[3].wait()
    loads[4].wait()
    projected = lax.dot_general(
        act[...].reshape(tp * own_ch, tokens),
        proj[...],
        (((0,), (0,)), ((), ())),
        preferred_element_type=F32,
    )
    mixed[...] = (resid[...].astype(F32) + projected).astype(BF)

    outg[...] = dot(pick[...], mixed[...]).astype(BF)
    rows[z, j, rows_of(x, cap), :] = outg[rows_of(s, cap), :]

    def offset(i):
        return ((i + 1) // 2) * (1 - 2 * ((i + 1) % 2))

    def dispatch(n, carry):
        i, dx = n // nx, n % nx
        e = ((z - offset(i) + nz) % nz) * nx + (x + dx) % nx
        remote(
            outg.at[rows_of(e, cap), :],
            rows.at[z, j, rows_of(x, cap), :],
            dsend,
            drecv.at[z],
            (e, j),
        )
        return carry

    lax.fori_loop(1, experts, dispatch, 0)

    def push(q, i, origin_y, hop, leg, sgn):
        ref = rows.at[q, 2 * origin_y + c]
        step = sgn * (1 - 2 * leg)
        where = (s, 2 * ((y + step + ny) % ny) + c)
        remote(ref, ref, rsend.at[i], rring.at[i, leg * ha + hop], where)

    def share(q, i, origin_y):
        ref = rows.at[q, 2 * origin_y + c]
        remote(ref, ref, rsend.at[i], rsib.at[i], (s, sib))

    def tick(t, carry):
        def at(stage, body):
            i = t - stage

            @pl.when((i >= 0) & (i < nz))
            def _():
                body(i, (z + offset(i) + nz) % nz, 1 - 2 * (i % 2))

        def rows_open(i, q, sgn):
            @pl.when(i == 0)
            def _():
                if nx > 1:
                    arrived(outg.at[pl.ds(0, (nx - 1) * cap), :], drecv.at[q])

            @pl.when(i > 0)
            def _():
                arrived(outg.at[pl.ds(0, nx * cap), :], drecv.at[q])

            push(q, i, y, 0, 0, sgn)
            if hb > 0:
                push(q, i, y, 0, 1, sgn)
            share(q, i, y)

        def rows_hop(h, i, q, sgn):
            for leg, reach in ((0, ha), (1, hb)):
                if h > reach:
                    continue
                origin = (y - sgn * (1 - 2 * leg) * h + 2 * ny) % ny
                arrived(rows.at[q, 2 * origin + c], rring.at[i, leg * ha + h - 1])
                if h < reach:
                    push(q, i, origin, h, leg, sgn)
                share(q, i, origin)

        def expert(i, q, sgn):
            @pl.when(i == 0)
            def _():
                loads[5].wait()
                loads[6].wait()
                arrived(wd.at[pl.ds(0, (tp - 1) * ffw), :], wdt_r)

            arrived(rows.at[q, pl.ds(0, ny)], rsib.at[i])
            r = jnp.concatenate([rows[q, b] for b in range(tp)], axis=1)
            g = dot(r, wg[...])
            u = dot(r, wu[...])
            h = ((g / (1.0 + jnp.exp(-g))) * u).astype(BF)
            for b in range(ny):
                w = jnp.concatenate([wdt[2 * b + c], wdt[2 * b + 1 - c]], axis=1)
                part = dot(h, w)
                own[i, b] = part[:, :width]
                give[i, b] = part[:, width:].astype(BF)
            remote(give.at[i], take.at[i], sib_s.at[i], sib_r.at[i], (s, sib))

        def mine(i, b):
            return own[i, b] + take[i, b].astype(F32)

        def sum_hop(m, i, q, sgn):
            if m == 1:
                arrived(take.at[i], sib_r.at[i])
            for leg, reach in ((0, ha), (1, hb)):
                if m > reach:
                    continue
                step = sgn * (1 - 2 * leg)
                k = reach - m + 1
                n = leg * ha + m - 1
                total = mine(i, (y + step * k + 2 * ny) % ny)
                if m > 1:
                    arrived(sumin.at[i, n - 1], sum_r.at[i, n - 1])
                    total = total + sumin[i, n - 1].astype(F32)
                sumout[i, n] = total.astype(BF)
                where = (s, 2 * ((y + step + ny) % ny) + c)
                remote(sumout.at[i, n], sumin.at[i, n], sum_s.at[i], sum_r.at[i, n], where)

        def finish(i, q, sgn):
            total = mine(i, y)
            for n in ([ha - 1, ny - 2] if hb > 0 else [ha - 1]):
                arrived(sumin.at[i, n], sum_r.at[i, n])
                total = total + sumin[i, n].astype(F32)
            res[i] = total.astype(BF)
            for xt in range(nx):
                tgt = q * nx + xt

                @pl.when(tgt == s)
                def _():
                    ret[rows_of(s, cap), :] = res[i, pl.ds(xt * cap, cap), :]

                @pl.when(tgt != s)
                def _():
                    remote(
                        res.at[i, pl.ds(xt * cap, cap), :],
                        ret.at[rows_of(s, cap), :],
                        bsend,
                        brecv,
                        (tgt, j),
                    )

        at(0, rows_open)
        for h in range(1, ha + 1):
            at(h, functools.partial(rows_hop, h))
        for m in range(1, ha + 1):
            at(ha + 1 + m, functools.partial(sum_hop, m))
        at(2 * ha + 2, finish)
        at(ha + 1, expert)
        return carry

    lax.fori_loop(0, nz + 2 * ha + 2, tick, 0)

    far = outg.at[pl.ds(0, (experts - 1) * cap), :]
    arrived(far, brecv)
    back = ret[...]
    routed = dot(pick0[...], back) * scales[:, 2:3] + dot(pick1[...], back) * scales[:, 3:4]
    out_ref[...] = (mixed[...].astype(F32) + routed).astype(BF)

    @pl.when(s < experts - 1)
    def _():
        arrived(halo, halo_s)

    arrived(wd.at[pl.ds(0, (tp - 1) * ffw), :], wdt_s)
    arrived(stats.at[pl.ds(0, tp - 1)], stat_s)
    arrived(act.at[pl.ds(0, 2 * ny - 1)], act_s)
    arrived(far, dsend)
    arrived(far, bsend)

    def drain(i, carry):
        arrived(rows.at[0, pl.ds(0, tp - 1)], rsend.at[i])
        arrived(give.at[0], sib_s.at[i])
        arrived(sumout.at[0], sum_s.at[i])
        return carry

    lax.fori_loop(0, nz, drain, 0)


def per_device(
    glu_value,
    glu_gate,
    conv_taps,
    norm_gain,
    out_proj,
    resid,
    expert_ids,
    route_logits,
    group_prob,
    w_gate,
    w_up,
    w_down,
):
    sp, tp = lax.axis_size("sp"), lax.axis_size("tp")
    nx = 4 if sp % 8 == 0 else 1
    nz, ny = sp // nx, tp // 2
    tokens, width = resid.shape
    cap = 4 * tokens // sp
    depth, ffw = w_gate.shape[1:]
    own_ch, taps = conv_taps.shape
    chunk = nx * cap
    dma = pltpu.SemaphoreType.DMA
    vmem = pl.BlockSpec(memory_space=pltpu.VMEM)
    hbm = pl.BlockSpec(memory_space=pl.ANY)
    dims = (nx, nz, ny, cap, taps, own_ch * tp)
    return pl.pallas_call(
        functools.partial(layer_kernel, dims),
        out_shape=jax.ShapeDtypeStruct((tokens, width), BF),
        in_specs=[hbm, hbm, vmem, vmem, hbm, hbm, vmem, vmem, vmem, hbm, hbm, hbm],
        out_specs=vmem,
        scratch_shapes=[
            pltpu.VMEM(glu_value.shape, BF),
            pltpu.VMEM(glu_gate.shape, BF),
            pltpu.VMEM(out_proj.shape, BF),
            pltpu.VMEM(resid.shape, BF),
            pltpu.VMEM((depth, ffw), BF),
            pltpu.VMEM((depth, ffw), BF),
            pltpu.VMEM(w_down.shape[1:], BF),
            pltpu.VMEM((tp, ffw, width), BF),
            pltpu.VMEM((32, LANES), F32),
            pltpu.VMEM((own_ch, LANES), BF),
            pltpu.VMEM((own_ch, LANES), BF),
            pltpu.VMEM((tp, 2, tokens), F32),
            pltpu.VMEM((tp, own_ch, tokens), BF),
            pltpu.VMEM((sp * cap, tokens), BF),
            pltpu.VMEM((tokens, sp * cap), BF),
            pltpu.VMEM((tokens, sp * cap), BF),
            pltpu.VMEM((tokens, 8), F32),
            pltpu.VMEM((tokens, width), BF),
            pltpu.VMEM((sp * cap, width), BF),
            pltpu.VMEM((nz, tp, chunk, width), BF),
            pltpu.VMEM((nz, ny, chunk, width), F32),
            pltpu.VMEM((nz, ny, chunk, width), BF),
            pltpu.VMEM((nz, ny, chunk, width), BF),
            pltpu.VMEM((nz, ny - 1, chunk, width), BF),
            pltpu.VMEM((nz, ny - 1, chunk, width), BF),
            pltpu.VMEM((nz, chunk, width), BF),
            pltpu.VMEM((sp * cap, width), BF),
            dma((7,)),
            dma(()),
            dma(()),
            dma(()),
            dma(()),
            dma(()),
            dma((ny,)),
            dma(()),
            dma(()),
            dma(()),
            dma(()),
            dma((nz,)),
            dma((nz, ny - 1)),
            dma((nz,)),
            dma((nz,)),
            dma((nz,)),
            dma((nz,)),
            dma((nz,)),
            dma((nz, ny - 1)),
            dma(()),
            dma(()),
        ],
        compiler_params=pltpu.CompilerParams(
            collective_id=0, has_side_effects=True, vmem_limit_bytes=63 * 1024 * 1024
        ),
    )(
        glu_value,
        glu_gate,
        conv_taps.T,
        norm_gain[None, :],
        out_proj,
        resid,
        expert_ids.T,
        route_logits.T,
        group_prob[None, :],
        w_gate,
        w_up,
        w_down,
    )


def solution(mesh):
    return jax.shard_map(
        per_device,
        mesh=mesh,
        in_specs=(
            P("tp", "sp"),
            P("tp", "sp"),
            P("tp", None),
            P("tp"),
            P(None, "tp"),
            P("sp", "tp"),
            P("sp", None),
            P("sp", None),
            P("sp"),
            P("sp", None, "tp"),
            P("sp", None, "tp"),
            P("sp", None, "tp"),
        ),
        out_specs=P("sp", "tp"),
        check_vma=False,
    )
```

```python
import functools
import jax
import jax.numpy as jnp
from jax import lax
from jax.experimental import pallas as pl
from jax.experimental.pallas import tpu as pltpu
from jax.sharding import PartitionSpec as P

BF = jnp.bfloat16
F32 = jnp.float32
MESH = pl.DeviceIdType.MESH
LANES = 128


def dot(a, b):
    return jnp.dot(a, b, preferred_element_type=F32)


def layer_kernel(
    dims,
    gv_hbm,
    gg_hbm,
    taps_ref,
    gain_ref,
    proj_hbm,
    resid_hbm,
    ids_ref,
    logits_ref,
    prob_ref,
    wg_hbm,
    wu_hbm,
    wd_hbm,
    out_ref,
    gv,
    gg,
    proj,
    resid,
    wg,
    wu,
    wd,
    wdt,
    tapcol,
    tail,
    halo,
    stats,
    act,
    pick,
    pick0,
    pick1,
    scales,
    mixed,
    outg,
    rows,
    own,
    give,
    take,
    sumout,
    sumin,
    res,
    ret,
    lsem,
    halo_s,
    halo_r,
    stat_s,
    stat_r,
    act_s,
    act_r,
    act_sib,
    wdt_s,
    wdt_r,
    dsend,
    drecv,
    rring,
    rsib,
    rsend,
    sib_s,
    sib_r,
    sum_s,
    sum_r,
    bsend,
    brecv,
):
    nx, nz, ny, cap, taps, channels = dims
    experts = nx * nz
    chunk = nx * cap
    tp = 2 * ny
    ha = ny // 2
    hb = ny - 1 - ha
    tokens, width = out_ref.shape
    own_ch = gv.shape[0]
    ffw = wg.shape[1]
    s = lax.axis_index("sp")
    j = lax.axis_index("tp")
    z, x = s // nx, s % nx
    y, c = j // 2, j % 2
    sib = 2 * y + (1 - c)

    def remote(src, dst, send, recv, where):
        pltpu.make_async_remote_copy(
            src_ref=src,
            dst_ref=dst,
            send_sem=send,
            recv_sem=recv,
            device_id=where,
            device_id_type=MESH,
        ).start()

    def arrived(ref, sem):
        pltpu.make_async_copy(ref, ref, sem).wait()

    def rows_of(n, size):
        return pl.ds(pl.multiple_of(n * size, size), size)

    loads = [
        pltpu.make_async_copy(a, b, lsem.at[n])
        for n, (a, b) in enumerate(
            (
                (gv_hbm, gv),
                (gg_hbm, gg),
                (wd_hbm.at[0], wd),
                (proj_hbm, proj),
                (resid_hbm, resid),
                (wg_hbm.at[0], wg),
                (wu_hbm.at[0], wu),
            )
        )
    ]
    for load in loads:
        load.start()

    barrier = pltpu.get_barrier_semaphore()

    def greet_sp(k, carry):
        pl.semaphore_signal(barrier, inc=1, device_id=((s + k) % experts, j), device_id_type=MESH)
        return carry

    def greet_tp(k, carry):
        pl.semaphore_signal(barrier, inc=1, device_id=(s, (j + k) % tp), device_id_type=MESH)
        return carry

    lax.fori_loop(1, experts, greet_sp, 0)
    lax.fori_loop(1, tp, greet_tp, 0)

    loads[0].wait()
    loads[1].wait()
    gated = (gv[...].astype(F32) * jax.nn.sigmoid(gg[...].astype(F32))).astype(BF)
    tail[...] = gated[:, tokens - LANES :]

    id0 = ids_ref[0:1, :]
    id1 = ids_ref[1:2, :]
    e_io = lax.broadcasted_iota(jnp.int32, (experts, tokens), 0)
    named = jnp.where((e_io == id0) | (e_io == id1), 1.0, 0.0)
    r_io = lax.broadcasted_iota(jnp.int32, (tokens, tokens), 0)
    c_io = lax.broadcasted_iota(jnp.int32, (tokens, tokens), 1)
    upper = jnp.where(r_io < c_io, 1.0, 0.0).astype(BF)
    before = dot(named.astype(BF), upper)
    slot0 = jnp.sum(jnp.where(e_io == id0, before, 0.0), axis=0, keepdims=True) + id0.astype(F32) * cap
    slot1 = jnp.sum(jnp.where(e_io == id1, before, 0.0), axis=0, keepdims=True) + id1.astype(F32) * cap
    s_io = lax.broadcasted_iota(jnp.int32, (experts * cap, tokens), 0).astype(F32)
    pick[...] = jnp.where((s_io == slot0) | (s_io == slot1), 1.0, 0.0).astype(BF)
    l0 = logits_ref[0:1, :]
    l1 = logits_ref[1:2, :]
    top = jnp.maximum(l0, l1)
    e0 = jnp.exp(l0 - top)
    e1 = jnp.exp(l1 - top)
    scale = prob_ref[...] / (e0 + e1)
    k_io = lax.broadcasted_iota(jnp.int32, (8, tokens), 0)
    stack = jnp.where(
        k_io == 0, slot0, jnp.where(k_io == 1, slot1, jnp.where(k_io == 2, e0 * scale, e1 * scale))
    )
    cols = stack.T
    scales[...] = cols
    t_io = lax.broadcasted_iota(jnp.int32, (tokens, experts * cap), 1).astype(F32)
    pick0[...] = jnp.where(t_io == cols[:, 0:1], 1.0, 0.0).astype(BF)
    pick1[...] = jnp.where(t_io == cols[:, 1:2], 1.0, 0.0).astype(BF)
    tapcol[...] = jnp.zeros_like(tapcol)
    tapcol[0:taps, 0:own_ch] = taps_ref[...]
    tapcol[taps : taps + 1, 0:own_ch] = gain_ref[...]
    tap = tapcol[...].T

    loads[2].wait()
    wdt[j] = wd[rows_of(j, ffw), :]

    pl.semaphore_wait(barrier, experts - 1 + tp - 1)

    def give_wd(peer_y, peer_c):
        peer = 2 * peer_y + peer_c
        remote(wd.at[rows_of(peer, ffw), :], wdt.at[j], wdt_s, wdt_r, (s, peer))

    def give_wd_at(reach):
        for d in sorted({reach % ny, (ny - reach) % ny}):
            give_wd((y + d) % ny, c)
            give_wd((y + d) % ny, 1 - c)

    @pl.when(s < experts - 1)
    def _():
        remote(tail, halo, halo_s, halo_r, ((s + 1) % experts, j))

    give_wd(y, 1 - c)
    give_wd_at(1)

    @pl.when(s == 0)
    def _():
        halo[...] = jnp.zeros_like(halo)

    @pl.when(s > 0)
    def _():
        arrived(halo, halo_r)

    padded = jnp.concatenate([halo[...], gated], axis=1).astype(F32)
    filtered = jnp.zeros((own_ch, tokens), F32)
    for o in range(taps):
        shift = taps - 1 - o
        moved = pltpu.roll(padded, shift, 1) if shift else padded
        filtered = filtered + tap[0:own_ch, o : o + 1] * moved[:, LANES:]
    stats[j, 0:1, :] = jnp.sum(filtered, axis=0, keepdims=True)
    stats[j, 1:2, :] = jnp.sum(filtered * filtered, axis=0, keepdims=True)

    def give_stats(k, carry):
        remote(stats.at[j], stats.at[j], stat_s, stat_r, (s, (j + k) % tp))
        return carry

    lax.fori_loop(1, tp, give_stats, 0)
    if ny > 2:
        give_wd_at(2)
    arrived(stats.at[pl.ds(0, tp - 1)], stat_r)
    totals = jnp.sum(stats[...], axis=0)
    mean = totals[0:1] / channels
    var = totals[1:2] / channels - mean * mean
    normed = (filtered - mean) * lax.rsqrt(var + 1e-05) * tap[0:own_ch, taps : taps + 1]
    act[j] = (normed / (1.0 + jnp.exp(-normed))).astype(BF)

    near = []
    for d in range(1, ha + 1):
        near.append(d)
        if ny - d != d:
            near.append(ny - d)
    for d in near:
        remote(act.at[j], act.at[j], act_s, act_r.at[d], (s, 2 * ((y + d) % ny) + c))
    remote(act.at[j], act.at[j], act_s, act_sib, (s, sib))
    for reach in range(3, ha + 1):
        give_wd_at(reach)
    for d in near:
        k = 2 * ((y + ny - d) % ny) + c
        arrived(act.at[k], act_r.at[d])
        remote(act.at[k], act.at[k], act_s, act_sib, (s, sib))
    arrived(act.at[pl.ds(0, ny)], act_sib)
    loads[3].wait()
    loads[4].wait()
    projected = lax.dot_general(
        act[...].reshape(tp * own_ch, tokens),
        proj[...],
        (((0,), (0,)), ((), ())),
        preferred_element_type=F32,
    )
    mixed[...] = (resid[...].astype(F32) + projected).astype(BF)

    outg[...] = dot(pick[...], mixed[...]).astype(BF)
    rows[z, j, rows_of(x, cap), :] = outg[rows_of(s, cap), :]

    def dispatch(n, carry):
        i, dx = n // nx, n % nx
        e = ((z - i + nz) % nz) * nx + (x + dx) % nx
        remote(
            outg.at[rows_of(e, cap), :],
            rows.at[z, j, rows_of(x, cap), :],
            dsend,
            drecv.at[z],
            (e, j),
        )
        return carry

    lax.fori_loop(1, experts, dispatch, 0)

    def push(q, i, origin_y, hop, leg, sgn):
        ref = rows.at[q, 2 * origin_y + c]
        step = sgn * (1 - 2 * leg)
        where = (s, 2 * ((y + step + ny) % ny) + c)
        remote(ref, ref, rsend.at[i], rring.at[i, leg * ha + hop], where)

    def share(q, i, origin_y):
        ref = rows.at[q, 2 * origin_y + c]
        remote(ref, ref, rsend.at[i], rsib.at[i], (s, sib))

    def tick(t, carry):
        def at(stage, body):
            i = t - 2 * stage

            @pl.when((i >= 0) & (i < nz))
            def _():
                body(i, (z + i) % nz, 1 - 2 * (i % 2))

        def rows_open(i, q, sgn):
            @pl.when(i == 0)
            def _():
                if nx > 1:
                    arrived(outg.at[pl.ds(0, (nx - 1) * cap), :], drecv.at[q])

            @pl.when(i > 0)
            def _():
                arrived(outg.at[pl.ds(0, nx * cap), :], drecv.at[q])

            push(q, i, y, 0, 0, sgn)
            if hb > 0:
                push(q, i, y, 0, 1, sgn)
            share(q, i, y)

        def rows_hop(h, i, q, sgn):
            for leg, reach in ((0, ha), (1, hb)):
                if h > reach:
                    continue
                origin = (y - sgn * (1 - 2 * leg) * h + 2 * ny) % ny
                arrived(rows.at[q, 2 * origin + c], rring.at[i, leg * ha + h - 1])
                if h < reach:
                    push(q, i, origin, h, leg, sgn)
                share(q, i, origin)

        def expert(i, q, sgn):
            @pl.when(i == 0)
            def _():
                loads[5].wait()
                loads[6].wait()
                arrived(wd.at[pl.ds(0, (tp - 1) * ffw), :], wdt_r)

            arrived(rows.at[q, pl.ds(0, ny)], rsib.at[i])
            r = jnp.concatenate([rows[q, b] for b in range(tp)], axis=1)
            g = dot(r, wg[...])
            u = dot(r, wu[...])
            h = ((g / (1.0 + jnp.exp(-g))) * u).astype(BF)
            for b in range(ny):
                w = jnp.concatenate([wdt[2 * b + c], wdt[2 * b + 1 - c]], axis=1)
                part = dot(h, w)
                own[i, b] = part[:, :width]
                give[i, b] = part[:, width:].astype(BF)
            remote(give.at[i], take.at[i], sib_s.at[i], sib_r.at[i], (s, sib))

        def mine(i, b):
            return own[i, b] + take[i, b].astype(F32)

        def sum_hop(m, i, q, sgn):
            if m == 1:
                arrived(take.at[i], sib_r.at[i])
            for leg, reach in ((0, ha), (1, hb)):
                if m > reach:
                    continue
                step = sgn * (1 - 2 * leg)
                k = reach - m + 1
                n = leg * ha + m - 1
                total = mine(i, (y + step * k + 2 * ny) % ny)
                if m > 1:
                    arrived(sumin.at[i, n - 1], sum_r.at[i, n - 1])
                    total = total + sumin[i, n - 1].astype(F32)
                sumout[i, n] = total.astype(BF)
                where = (s, 2 * ((y + step + ny) % ny) + c)
                remote(sumout.at[i, n], sumin.at[i, n], sum_s.at[i], sum_r.at[i, n], where)

        def finish(i, q, sgn):
            total = mine(i, y)
            for n in ([ha - 1, ny - 2] if hb > 0 else [ha - 1]):
                arrived(sumin.at[i, n], sum_r.at[i, n])
                total = total + sumin[i, n].astype(F32)
            res[i] = total.astype(BF)
            for xt in range(nx):
                tgt = q * nx + xt

                @pl.when(tgt == s)
                def _():
                    ret[rows_of(s, cap), :] = res[i, pl.ds(xt * cap, cap), :]

                @pl.when(tgt != s)
                def _():
                    remote(
                        res.at[i, pl.ds(xt * cap, cap), :],
                        ret.at[rows_of(s, cap), :],
                        bsend,
                        brecv,
                        (tgt, j),
                    )

        at(0, rows_open)
        for h in range(1, ha + 1):
            at(h, functools.partial(rows_hop, h))
        for m in range(1, ha + 1):
            at(ha + 1 + m, functools.partial(sum_hop, m))
        at(2 * ha + 2, finish)
        at(ha + 1, expert)
        return carry

    lax.fori_loop(0, nz + 2 * (2 * ha + 2), tick, 0)

    far = outg.at[pl.ds(0, (experts - 1) * cap), :]
    arrived(far, brecv)
    back = ret[...]
    routed = dot(pick0[...], back) * scales[:, 2:3] + dot(pick1[...], back) * scales[:, 3:4]
    out_ref[...] = (mixed[...].astype(F32) + routed).astype(BF)

    @pl.when(s < experts - 1)
    def _():
        arrived(halo, halo_s)

    arrived(wd.at[pl.ds(0, (tp - 1) * ffw), :], wdt_s)
    arrived(stats.at[pl.ds(0, tp - 1)], stat_s)
    arrived(act.at[pl.ds(0, 2 * ny - 1)], act_s)
    arrived(far, dsend)
    arrived(far, bsend)

    def drain(i, carry):
        arrived(rows.at[0, pl.ds(0, tp - 1)], rsend.at[i])
        arrived(give.at[0], sib_s.at[i])
        arrived(sumout.at[0], sum_s.at[i])
        return carry

    lax.fori_loop(0, nz, drain, 0)


def per_device(
    glu_value,
    glu_gate,
    conv_taps,
    norm_gain,
    out_proj,
    resid,
    expert_ids,
    route_logits,
    group_prob,
    w_gate,
    w_up,
    w_down,
):
    sp, tp = lax.axis_size("sp"), lax.axis_size("tp")
    nx = 4 if sp % 8 == 0 else 1
    nz, ny = sp // nx, tp // 2
    tokens, width = resid.shape
    cap = 4 * tokens // sp
    depth, ffw = w_gate.shape[1:]
    own_ch, taps = conv_taps.shape
    chunk = nx * cap
    dma = pltpu.SemaphoreType.DMA
    vmem = pl.BlockSpec(memory_space=pltpu.VMEM)
    hbm = pl.BlockSpec(memory_space=pl.ANY)
    dims = (nx, nz, ny, cap, taps, own_ch * tp)
    return pl.pallas_call(
        functools.partial(layer_kernel, dims),
        out_shape=jax.ShapeDtypeStruct((tokens, width), BF),
        in_specs=[hbm, hbm, vmem, vmem, hbm, hbm, vmem, vmem, vmem, hbm, hbm, hbm],
        out_specs=vmem,
        scratch_shapes=[
            pltpu.VMEM(glu_value.shape, BF),
            pltpu.VMEM(glu_gate.shape, BF),
            pltpu.VMEM(out_proj.shape, BF),
            pltpu.VMEM(resid.shape, BF),
            pltpu.VMEM((depth, ffw), BF),
            pltpu.VMEM((depth, ffw), BF),
            pltpu.VMEM(w_down.shape[1:], BF),
            pltpu.VMEM((tp, ffw, width), BF),
            pltpu.VMEM((32, LANES), F32),
            pltpu.VMEM((own_ch, LANES), BF),
            pltpu.VMEM((own_ch, LANES), BF),
            pltpu.VMEM((tp, 2, tokens), F32),
            pltpu.VMEM((tp, own_ch, tokens), BF),
            pltpu.VMEM((sp * cap, tokens), BF),
            pltpu.VMEM((tokens, sp * cap), BF),
            pltpu.VMEM((tokens, sp * cap), BF),
            pltpu.VMEM((tokens, 8), F32),
            pltpu.VMEM((tokens, width), BF),
            pltpu.VMEM((sp * cap, width), BF),
            pltpu.VMEM((nz, tp, chunk, width), BF),
            pltpu.VMEM((nz, ny, chunk, width), F32),
            pltpu.VMEM((nz, ny, chunk, width), BF),
            pltpu.VMEM((nz, ny, chunk, width), BF),
            pltpu.VMEM((nz, ny - 1, chunk, width), BF),
            pltpu.VMEM((nz, ny - 1, chunk, width), BF),
            pltpu.VMEM((nz, chunk, width), BF),
            pltpu.VMEM((sp * cap, width), BF),
            dma((7,)),
            dma(()),
            dma(()),
            dma(()),
            dma(()),
            dma(()),
            dma((ny,)),
            dma(()),
            dma(()),
            dma(()),
            dma(()),
            dma((nz,)),
            dma((nz, ny - 1)),
            dma((nz,)),
            dma((nz,)),
            dma((nz,)),
            dma((nz,)),
            dma((nz,)),
            dma((nz, ny - 1)),
            dma(()),
            dma(()),
        ],
        compiler_params=pltpu.CompilerParams(
            collective_id=0, has_side_effects=True, vmem_limit_bytes=63 * 1024 * 1024
        ),
    )(
        glu_value,
        glu_gate,
        conv_taps.T,
        norm_gain[None, :],
        out_proj,
        resid,
        expert_ids.T,
        route_logits.T,
        group_prob[None, :],
        w_gate,
        w_up,
        w_down,
    )


def solution(mesh):
    return jax.shard_map(
        per_device,
        mesh=mesh,
        in_specs=(
            P("tp", "sp"),
            P("tp", "sp"),
            P("tp", None),
            P("tp"),
            P(None, "tp"),
            P("sp", "tp"),
            P("sp", None),
            P("sp", None),
            P("sp"),
            P("sp", None, "tp"),
            P("sp", None, "tp"),
            P("sp", None, "tp"),
        ),
        out_specs=P("sp", "tp"),
        check_vma=False,
    )
```

```python
import functools
import jax
import jax.numpy as jnp
from jax import lax
from jax.experimental import pallas as pl
from jax.experimental.pallas import tpu as pltpu
from jax.sharding import PartitionSpec as P

BF = jnp.bfloat16
F32 = jnp.float32
MESH = pl.DeviceIdType.MESH
LANES = 128


def dot(a, b):
    return jnp.dot(a, b, preferred_element_type=F32)


def layer_kernel(
    dims,
    gv_hbm,
    gg_hbm,
    taps_ref,
    gain_ref,
    proj_hbm,
    resid_hbm,
    ids_ref,
    logits_ref,
    prob_ref,
    wg_hbm,
    wu_hbm,
    wd_hbm,
    out_ref,
    gv,
    gg,
    proj,
    resid,
    wg,
    wu,
    wd,
    wdt,
    tapcol,
    tail,
    halo,
    stats,
    act,
    pick,
    pick0,
    pick1,
    scales,
    mixed,
    outg,
    rows,
    own,
    give,
    take,
    sumout,
    sumin,
    res,
    ret,
    lsem,
    halo_s,
    halo_r,
    stat_s,
    stat_r,
    act_s,
    act_r,
    act_sib,
    relay,
    relay_s,
    relay_r,
    wdt_s,
    wdt_r,
    dsend,
    drecv,
    rring,
    rsib,
    rsend,
    sib_s,
    sib_r,
    sum_s,
    sum_r,
    bsend,
    brecv,
):
    nx, nz, ny, cap, taps, channels = dims
    experts = nx * nz
    chunk = nx * cap
    tp = 2 * ny
    ha = ny // 2
    hb = ny - 1 - ha
    tokens, width = out_ref.shape
    own_ch = gv.shape[0]
    ffw = wg.shape[1]
    s = lax.axis_index("sp")
    j = lax.axis_index("tp")
    z, x = lax.div(s, nx), lax.rem(s, nx)
    y, c = lax.div(j, 2), lax.rem(j, 2)
    sib = 2 * y + (1 - c)

    def remote(src, dst, send, recv, where):
        pltpu.make_async_remote_copy(
            src_ref=src,
            dst_ref=dst,
            send_sem=send,
            recv_sem=recv,
            device_id=where,
            device_id_type=MESH,
        ).start()

    def arrived(ref, sem):
        pltpu.make_async_copy(ref, ref, sem).wait()

    def rows_of(n, size):
        return pl.ds(pl.multiple_of(n * size, size), size)

    loads = [
        pltpu.make_async_copy(a, b, lsem.at[n])
        for n, (a, b) in enumerate(
            (
                (gv_hbm, gv),
                (gg_hbm, gg),
                (wd_hbm.at[0], wd),
                (proj_hbm, proj),
                (resid_hbm, resid),
                (wg_hbm.at[0], wg),
                (wu_hbm.at[0], wu),
            )
        )
    ]
    for load in loads:
        load.start()

    barrier = pltpu.get_barrier_semaphore()

    for k in sorted(range(1, experts), key=lambda k: -min(k // nx, nz - k // nx)):
        peer = (lax.rem(s + k, experts), j)
        pl.semaphore_signal(barrier, inc=1, device_id=peer, device_id_type=MESH)
    far_first = sorted(range(1, tp), key=lambda k: -min(k // 2, ny - k // 2))
    for k in far_first:
        peer = (s, lax.rem(j + k, tp))
        pl.semaphore_signal(barrier, inc=1, device_id=peer, device_id_type=MESH)

    loads[0].wait()
    loads[1].wait()
    gated = (gv[...].astype(F32) * jax.nn.sigmoid(gg[...].astype(F32))).astype(BF)
    tail[...] = gated[:, tokens - LANES :]

    id0 = ids_ref[0:1, :]
    id1 = ids_ref[1:2, :]
    e_io = lax.broadcasted_iota(jnp.int32, (experts, tokens), 0)
    named = jnp.where((e_io == id0) | (e_io == id1), 1.0, 0.0)
    r_io = lax.broadcasted_iota(jnp.int32, (tokens, tokens), 0)
    c_io = lax.broadcasted_iota(jnp.int32, (tokens, tokens), 1)
    upper = jnp.where(r_io < c_io, 1.0, 0.0).astype(BF)
    before = dot(named.astype(BF), upper)
    slot0 = jnp.sum(jnp.where(e_io == id0, before, 0.0), axis=0, keepdims=True) + id0.astype(F32) * cap
    slot1 = jnp.sum(jnp.where(e_io == id1, before, 0.0), axis=0, keepdims=True) + id1.astype(F32) * cap
    s_io = lax.broadcasted_iota(jnp.int32, (experts * cap, tokens), 0).astype(F32)
    pick[...] = jnp.where((s_io == slot0) | (s_io == slot1), 1.0, 0.0).astype(BF)
    l0 = logits_ref[0:1, :]
    l1 = logits_ref[1:2, :]
    top = jnp.maximum(l0, l1)
    e0 = jnp.exp(l0 - top)
    e1 = jnp.exp(l1 - top)
    scale = prob_ref[...] / (e0 + e1)
    k_io = lax.broadcasted_iota(jnp.int32, (8, tokens), 0)
    stack = jnp.where(
        k_io == 0, slot0, jnp.where(k_io == 1, slot1, jnp.where(k_io == 2, e0 * scale, e1 * scale))
    )
    cols = stack.T
    scales[...] = cols
    t_io = lax.broadcasted_iota(jnp.int32, (tokens, experts * cap), 1).astype(F32)
    pick0[...] = jnp.where(t_io == cols[:, 0:1], 1.0, 0.0).astype(BF)
    pick1[...] = jnp.where(t_io == cols[:, 1:2], 1.0, 0.0).astype(BF)
    tapcol[...] = jnp.zeros_like(tapcol)
    tapcol[0:taps, 0:own_ch] = taps_ref[...]
    tapcol[taps : taps + 1, 0:own_ch] = gain_ref[...]
    tap = tapcol[...].T

    loads[2].wait()
    wdt[j] = wd[rows_of(j, ffw), :]

    pl.semaphore_wait(barrier, experts - 1 + tp - 1)

    def give_wd(peer_y, peer_c):
        peer = 2 * peer_y + peer_c
        remote(wd.at[rows_of(peer, ffw), :], wdt.at[j], wdt_s, wdt_r, (s, peer))

    def give_wd_at(reach):
        for d in sorted({reach % ny, (ny - reach) % ny}):
            give_wd((y + d) % ny, c)
            give_wd((y + d) % ny, 1 - c)

    halfway = ny // 4
    lean = 1 - 2 * c
    before_y, after_y = (y - lean * halfway + ny) % ny, (y + lean * halfway + ny) % ny
    across = (y + ha) % ny

    def give_wd_across():
        for n, peer_c in enumerate((c, 1 - c)):
            block = wd.at[rows_of(2 * across + peer_c, ffw), :]
            remote(block, relay.at[n], relay_s, relay_r, (s, 2 * after_y + c))

    def relay_wd():
        arrived(relay, relay_r)
        for n, peer_c in enumerate((c, 1 - c)):
            remote(relay.at[n], wdt.at[2 * before_y + c], wdt_s, wdt_r, (s, 2 * after_y + peer_c))

    @pl.when(s < experts - 1)
    def _():
        remote(tail, halo, halo_s, halo_r, ((s + 1) % experts, j))

    give_wd(y, 1 - c)
    give_wd_at(1)

    @pl.when(s == 0)
    def _():
        halo[...] = jnp.zeros_like(halo)

    @pl.when(s > 0)
    def _():
        arrived(halo, halo_r)

    padded = jnp.concatenate([halo[...], gated], axis=1).astype(F32)
    filtered = jnp.zeros((own_ch, tokens), F32)
    for o in range(taps):
        shift = taps - 1 - o
        moved = pltpu.roll(padded, shift, 1) if shift else padded
        filtered = filtered + tap[0:own_ch, o : o + 1] * moved[:, LANES:]
    stats[j, 0:1, :] = jnp.sum(filtered, axis=0, keepdims=True)
    stats[j, 1:2, :] = jnp.sum(filtered * filtered, axis=0, keepdims=True)

    for k in far_first:
        remote(stats.at[j], stats.at[j], stat_s, stat_r, (s, lax.rem(j + k, tp)))
    for reach in range(2, ha - 1):
        give_wd_at(reach)
    arrived(stats.at[pl.ds(0, tp - 1)], stat_r)
    totals = jnp.sum(stats[...], axis=0)
    mean = totals[0:1] / channels
    var = totals[1:2] / channels - mean * mean
    normed = (filtered - mean) * lax.rsqrt(var + 1e-05) * tap[0:own_ch, taps : taps + 1]
    act[j] = (normed / (1.0 + jnp.exp(-normed))).astype(BF)

    def act_from(d):
        return act.at[2 * ((y - d + 2 * ny) % ny) + c]

    def send_act(d, reach):
        ref = act_from(d)
        remote(ref, ref, act_s, act_r.at[(d + reach) % ny], (s, 2 * ((y + reach + ny) % ny) + c))

    def share_act(d):
        ref = act_from(d)
        arrived(ref, act_r.at[d % ny])
        remote(ref, ref, act_s, act_sib, (s, sib))

    for reach in range(halfway, 0, -1):
        send_act(0, reach)
        send_act(0, -reach)
    remote(act.at[j], act.at[j], act_s, act_sib, (s, sib))
    for side in (1, -1):
        share_act(side * halfway)
        for reach in range(1, halfway):
            send_act(side * halfway, side * reach)

        @pl.when(lean == side)
        def _():
            send_act(side * halfway, side * halfway)

    give_wd_across()
    if ha > 2:
        give_wd_at(ha - 1)
    for d in range(1, halfway):
        share_act(d)
        share_act(-d)
    for d in range(halfway + 1, ha):
        share_act(d)
        share_act(-d)
    share_act(ha)
    arrived(act.at[pl.ds(0, ny)], act_sib)
    loads[3].wait()
    loads[4].wait()
    projected = lax.dot_general(
        act[...].reshape(tp * own_ch, tokens),
        proj[...],
        (((0,), (0,)), ((), ())),
        preferred_element_type=F32,
    )
    mixed[...] = (resid[...].astype(F32) + projected).astype(BF)

    outg[...] = dot(pick[...], mixed[...]).astype(BF)
    rows[z, c, y, rows_of(x, cap), :] = outg[rows_of(s, cap), :]

    for i in range(nz):
        zt = lax.rem(z + (nz - i), nz)
        for dx in range(nx):
            if i + dx == 0:
                continue
            e = zt * nx + lax.rem(x + dx, nx)
            remote(
                outg.at[rows_of(e, cap), :],
                rows.at[z, c, y, rows_of(x, cap), :],
                dsend,
                drecv.at[z],
                (e, j),
            )

    relay_wd()
    above = 2 * lax.rem(y + 1, ny) + c
    below = 2 * lax.rem(y + (ny - 1), ny) + c

    def toward(odd, leg):
        return (s, above + (odd if leg == 0 else 1 - odd) * (below - above))

    def chip(step, k):
        return lax.rem(y + step * k + ny, ny)

    def push(q, i, origin_y, hop, leg, odd):
        ref = rows.at[q, c, origin_y]
        remote(ref, ref, rsend.at[i], rring.at[i, leg * ha + hop], toward(odd, leg))

    def tick(t, carry):
        def at(stage, body):
            i = t - stage

            @pl.when((i >= 0) & (i < nz))
            def _():
                body(i, lax.rem(z + i, nz), lax.rem(i, 2))

        def rows_open(i, q, odd):
            @pl.when(i == 0)
            def _():
                if nx > 1:
                    arrived(outg.at[pl.ds(0, (nx - 1) * cap), :], drecv.at[q])

            @pl.when(i > 0)
            def _():
                arrived(outg.at[pl.ds(0, nx * cap), :], drecv.at[q])

            push(q, i, y, 0, 0, odd)
            if hb > 0:
                push(q, i, y, 0, 1, odd)

        def rows_hop(h, i, q, odd):
            for leg, reach in ((0, ha), (1, hb)):
                if h > reach:
                    continue
                origin = chip((2 * odd - 1) * (1 - 2 * leg), h)
                arrived(rows.at[q, c, origin], rring.at[i, leg * ha + h - 1])
                if h < reach:
                    push(q, i, origin, h, leg, odd)
            if h == ha:
                remote(rows.at[q, c], rows.at[q, c], rsend.at[i], rsib.at[i], (s, sib))

        def expert(i, q, odd):
            @pl.when(i == 0)
            def _():
                loads[5].wait()
                loads[6].wait()
                arrived(wd.at[pl.ds(0, (tp - 1) * ffw), :], wdt_r)

            arrived(rows.at[q, 0], rsib.at[i])
            r = jnp.concatenate([rows[q, b % 2, b // 2] for b in range(tp)], axis=1)
            g = dot(r, wg[...])
            u = dot(r, wu[...])
            h = ((g / (1.0 + jnp.exp(-g))) * u).astype(BF)
            for b in range(ny):
                w = jnp.concatenate([wdt[2 * b + c], wdt[2 * b + 1 - c]], axis=1)
                part = dot(h, w)
                own[i, b] = part[:, :width]
                give[i, b] = part[:, width:].astype(BF)
            remote(give.at[i], take.at[i], sib_s.at[i], sib_r.at[i], (s, sib))

        def mine(i, b):
            return own[i, b] + take[i, b].astype(F32)

        def sum_hop(m, i, q, odd):
            if m == 1:
                arrived(take.at[i], sib_r.at[i])
            for leg, reach in ((0, ha), (1, hb)):
                if m > reach:
                    continue
                k = reach - m + 1
                n = leg * ha + m - 1
                total = mine(i, chip((1 - 2 * odd) * (1 - 2 * leg), k))
                if m > 1:
                    arrived(sumin.at[i, n - 1], sum_r.at[i, n - 1])
                    total = total + sumin[i, n - 1].astype(F32)
                sumout[i, n] = total.astype(BF)
                ref = sumout.at[i, n]
                remote(ref, sumin.at[i, n], sum_s.at[i], sum_r.at[i, n], toward(odd, leg))

        def finish(i, q, odd):
            total = mine(i, y)
            for n in ([ha - 1, ny - 2] if hb > 0 else [ha - 1]):
                arrived(sumin.at[i, n], sum_r.at[i, n])
                total = total + sumin[i, n].astype(F32)
            res[i] = total.astype(BF)
            for xt in range(nx):
                tgt = q * nx + xt

                @pl.when(tgt == s)
                def _():
                    ret[rows_of(s, cap), :] = res[i, pl.ds(xt * cap, cap), :]

                @pl.when(tgt != s)
                def _():
                    remote(
                        res.at[i, pl.ds(xt * cap, cap), :],
                        ret.at[rows_of(s, cap), :],
                        bsend,
                        brecv,
                        (tgt, j),
                    )

        last = 2 * ha + 2
        at(2 * last - 2, finish)
        for m in range(ha, 0, -1):
            at(last + 2 * (m - 1), functools.partial(sum_hop, m))
        for h in range(ha, 0, -1):
            at(2 * h, functools.partial(rows_hop, h))
        at(0, rows_open)
        at(last - 1, expert)
        return carry

    lax.fori_loop(0, nz + 4 * ha + 2, tick, 0)

    far = outg.at[pl.ds(0, (experts - 1) * cap), :]
    arrived(far, brecv)
    back = ret[...]
    routed = dot(pick0[...], back) * scales[:, 2:3] + dot(pick1[...], back) * scales[:, 3:4]
    out_ref[...] = (mixed[...].astype(F32) + routed).astype(BF)

    @pl.when(s < experts - 1)
    def _():
        arrived(halo, halo_s)

    arrived(wd.at[pl.ds(0, (tp - 1) * ffw), :], wdt_s)
    arrived(relay, relay_s)
    arrived(stats.at[pl.ds(0, tp - 1)], stat_s)
    arrived(act.at[pl.ds(0, 2 * ny - 1)], act_s)
    arrived(far, dsend)
    arrived(far, bsend)

    def drain(i, carry):
        arrived(rows.at[0, 0], rsend.at[i])
        arrived(rows.at[0, 0, pl.ds(0, ny - 1)], rsend.at[i])
        arrived(give.at[0], sib_s.at[i])
        arrived(sumout.at[0], sum_s.at[i])
        return carry

    lax.fori_loop(0, nz, drain, 0)


def per_device(
    glu_value,
    glu_gate,
    conv_taps,
    norm_gain,
    out_proj,
    resid,
    expert_ids,
    route_logits,
    group_prob,
    w_gate,
    w_up,
    w_down,
):
    sp, tp = lax.axis_size("sp"), lax.axis_size("tp")
    nx = 4 if sp % 8 == 0 else 1
    nz, ny = sp // nx, tp // 2
    tokens, width = resid.shape
    cap = 4 * tokens // sp
    depth, ffw = w_gate.shape[1:]
    own_ch, taps = conv_taps.shape
    chunk = nx * cap
    dma = pltpu.SemaphoreType.DMA
    vmem = pl.BlockSpec(memory_space=pltpu.VMEM)
    hbm = pl.BlockSpec(memory_space=pl.ANY)
    dims = (nx, nz, ny, cap, taps, own_ch * tp)
    return pl.pallas_call(
        functools.partial(layer_kernel, dims),
        out_shape=jax.ShapeDtypeStruct((tokens, width), BF),
        in_specs=[hbm, hbm, vmem, vmem, hbm, hbm, vmem, vmem, vmem, hbm, hbm, hbm],
        out_specs=vmem,
        scratch_shapes=[
            pltpu.VMEM(glu_value.shape, BF),
            pltpu.VMEM(glu_gate.shape, BF),
            pltpu.VMEM(out_proj.shape, BF),
            pltpu.VMEM(resid.shape, BF),
            pltpu.VMEM((depth, ffw), BF),
            pltpu.VMEM((depth, ffw), BF),
            pltpu.VMEM(w_down.shape[1:], BF),
            pltpu.VMEM((tp, ffw, width), BF),
            pltpu.VMEM((32, LANES), F32),
            pltpu.VMEM((own_ch, LANES), BF),
            pltpu.VMEM((own_ch, LANES), BF),
            pltpu.VMEM((tp, 2, tokens), F32),
            pltpu.VMEM((tp, own_ch, tokens), BF),
            pltpu.VMEM((sp * cap, tokens), BF),
            pltpu.VMEM((tokens, sp * cap), BF),
            pltpu.VMEM((tokens, sp * cap), BF),
            pltpu.VMEM((tokens, 8), F32),
            pltpu.VMEM((tokens, width), BF),
            pltpu.VMEM((sp * cap, width), BF),
            pltpu.VMEM((nz, 2, ny, chunk, width), BF),
            pltpu.VMEM((nz, ny, chunk, width), F32),
            pltpu.VMEM((nz, ny, chunk, width), BF),
            pltpu.VMEM((nz, ny, chunk, width), BF),
            pltpu.VMEM((nz, ny - 1, chunk, width), BF),
            pltpu.VMEM((nz, ny - 1, chunk, width), BF),
            pltpu.VMEM((nz, chunk, width), BF),
            pltpu.VMEM((sp * cap, width), BF),
            dma((7,)),
            dma(()),
            dma(()),
            dma(()),
            dma(()),
            dma(()),
            dma((ny,)),
            dma(()),
            pltpu.VMEM((2, ffw, width), BF),
            dma(()),
            dma(()),
            dma(()),
            dma(()),
            dma(()),
            dma((nz,)),
            dma((nz, ny - 1)),
            dma((nz,)),
            dma((nz,)),
            dma((nz,)),
            dma((nz,)),
            dma((nz,)),
            dma((nz, ny - 1)),
            dma(()),
            dma(()),
        ],
        compiler_params=pltpu.CompilerParams(
            collective_id=0, has_side_effects=True, vmem_limit_bytes=63 * 1024 * 1024
        ),
    )(
        glu_value,
        glu_gate,
        conv_taps.T,
        norm_gain[None, :],
        out_proj,
        resid,
        expert_ids.T,
        route_logits.T,
        group_prob[None, :],
        w_gate,
        w_up,
        w_down,
    )


def solution(mesh):
    return jax.shard_map(
        per_device,
        mesh=mesh,
        in_specs=(
            P("tp", "sp"),
            P("tp", "sp"),
            P("tp", None),
            P("tp"),
            P(None, "tp"),
            P("sp", "tp"),
            P("sp", None),
            P("sp", None),
            P("sp"),
            P("sp", None, "tp"),
            P("sp", None, "tp"),
            P("sp", None, "tp"),
        ),
        out_specs=P("sp", "tp"),
        check_vma=False,
    )
```

```python
import functools
import jax
import jax.numpy as jnp
from jax import lax
from jax.experimental import pallas as pl
from jax.experimental.pallas import tpu as pltpu
from jax.sharding import PartitionSpec as P

BF = jnp.bfloat16
F32 = jnp.float32
MESH = pl.DeviceIdType.MESH
LANES = 128


def dot(a, b):
    return jnp.dot(a, b, preferred_element_type=F32)


def layer_kernel(
    dims,
    gv_hbm,
    gg_hbm,
    taps_ref,
    gain_ref,
    proj_hbm,
    resid_hbm,
    ids_ref,
    logits_ref,
    prob_ref,
    wg_hbm,
    wu_hbm,
    wd_hbm,
    out_ref,
    gv,
    gg,
    proj,
    resid,
    wg,
    wu,
    wd,
    wdt,
    tapcol,
    tail,
    halo,
    stats,
    act,
    pick,
    pick0,
    pick1,
    scales,
    mixed,
    outg,
    rows,
    own,
    give,
    take,
    sumout,
    sumin,
    res,
    ret,
    lsem,
    halo_s,
    halo_r,
    stat_s,
    stat_r,
    act_s,
    act_r,
    act_sib,
    relay,
    relay_s,
    relay_r,
    wdt_s,
    wdt_r,
    dsend,
    drecv,
    rring,
    rsib,
    rsend,
    sib_s,
    sib_r,
    sum_s,
    sum_r,
    bsend,
    brecv,
):
    nx, nz, ny, cap, taps, channels = dims
    experts = nx * nz
    chunk = nx * cap
    tp = 2 * ny
    ha = ny // 2
    hb = ny - 1 - ha
    tokens, width = out_ref.shape
    own_ch = gv.shape[0]
    ffw = wg.shape[1]
    s = lax.axis_index("sp")
    j = lax.axis_index("tp")
    z, x = lax.div(s, nx), lax.rem(s, nx)
    y, c = lax.div(j, 2), lax.rem(j, 2)
    sib = 2 * y + (1 - c)

    def remote(src, dst, send, recv, where):
        pltpu.make_async_remote_copy(
            src_ref=src,
            dst_ref=dst,
            send_sem=send,
            recv_sem=recv,
            device_id=where,
            device_id_type=MESH,
        ).start()

    def arrived(ref, sem):
        pltpu.make_async_copy(ref, ref, sem).wait()

    def rows_of(n, size):
        return pl.ds(pl.multiple_of(n * size, size), size)

    loads = [
        pltpu.make_async_copy(a, b, lsem.at[n])
        for n, (a, b) in enumerate(
            (
                (gv_hbm, gv),
                (gg_hbm, gg),
                (wd_hbm.at[0], wd),
                (proj_hbm, proj),
                (resid_hbm, resid),
                (wg_hbm.at[0], wg),
                (wu_hbm.at[0], wu),
            )
        )
    ]
    barrier = pltpu.get_barrier_semaphore()

    for k in sorted(range(1, experts), key=lambda k: -min(k // nx, nz - k // nx)):
        peer = (lax.rem(s + k, experts), j)
        pl.semaphore_signal(barrier, inc=1, device_id=peer, device_id_type=MESH)
    far_first = sorted(range(1, tp), key=lambda k: -min(k // 2, ny - k // 2))
    for k in far_first:
        peer = (s, lax.rem(j + k, tp))
        pl.semaphore_signal(barrier, inc=1, device_id=peer, device_id_type=MESH)

    for load in loads:
        load.start()

    loads[0].wait()
    loads[1].wait()
    gated = (gv[...].astype(F32) * jax.nn.sigmoid(gg[...].astype(F32))).astype(BF)
    tail[...] = gated[:, tokens - LANES :]

    id0 = ids_ref[0:1, :]
    id1 = ids_ref[1:2, :]
    e_io = lax.broadcasted_iota(jnp.int32, (experts, tokens), 0)
    named = jnp.where((e_io == id0) | (e_io == id1), 1.0, 0.0)
    r_io = lax.broadcasted_iota(jnp.int32, (tokens, tokens), 0)
    c_io = lax.broadcasted_iota(jnp.int32, (tokens, tokens), 1)
    upper = jnp.where(r_io < c_io, 1.0, 0.0).astype(BF)
    before = dot(named.astype(BF), upper)
    slot0 = jnp.sum(jnp.where(e_io == id0, before, 0.0), axis=0, keepdims=True) + id0.astype(F32) * cap
    slot1 = jnp.sum(jnp.where(e_io == id1, before, 0.0), axis=0, keepdims=True) + id1.astype(F32) * cap
    s_io = lax.broadcasted_iota(jnp.int32, (experts * cap, tokens), 0).astype(F32)
    pick[...] = jnp.where((s_io == slot0) | (s_io == slot1), 1.0, 0.0).astype(BF)
    l0 = logits_ref[0:1, :]
    l1 = logits_ref[1:2, :]
    top = jnp.maximum(l0, l1)
    e0 = jnp.exp(l0 - top)
    e1 = jnp.exp(l1 - top)
    scale = prob_ref[...] / (e0 + e1)
    k_io = lax.broadcasted_iota(jnp.int32, (8, tokens), 0)
    stack = jnp.where(
        k_io == 0, slot0, jnp.where(k_io == 1, slot1, jnp.where(k_io == 2, e0 * scale, e1 * scale))
    )
    cols = stack.T
    scales[...] = cols
    t_io = lax.broadcasted_iota(jnp.int32, (tokens, experts * cap), 1).astype(F32)
    pick0[...] = jnp.where(t_io == cols[:, 0:1], 1.0, 0.0).astype(BF)
    pick1[...] = jnp.where(t_io == cols[:, 1:2], 1.0, 0.0).astype(BF)
    tapcol[...] = jnp.zeros_like(tapcol)
    tapcol[0:taps, 0:own_ch] = taps_ref[...]
    tapcol[taps : taps + 1, 0:own_ch] = gain_ref[...]
    tap = tapcol[...].T

    def convolve(block):
        total = jnp.zeros((own_ch, block.shape[1] - LANES), F32)
        for o in range(taps):
            shift = taps - 1 - o
            moved = pltpu.roll(block, shift, 1) if shift else block
            total = total + tap[0:own_ch, o : o + 1] * moved[:, LANES:]
        return total

    later = convolve(gated.astype(F32))

    loads[2].wait()
    wdt[j] = wd[rows_of(j, ffw), :]

    pl.semaphore_wait(barrier, experts - 1 + tp - 1)

    def give_wd(peer_y, peer_c):
        peer = 2 * peer_y + peer_c
        remote(wd.at[rows_of(peer, ffw), :], wdt.at[j], wdt_s, wdt_r, (s, peer))

    def give_wd_at(reach):
        for d in sorted({reach % ny, (ny - reach) % ny}):
            give_wd((y + d) % ny, c)
            give_wd((y + d) % ny, 1 - c)

    halfway = ny // 4
    lean = 1 - 2 * c
    before_y, after_y = (y - lean * halfway + ny) % ny, (y + lean * halfway + ny) % ny
    across = (y + ha) % ny

    def give_wd_across():
        for n, peer_c in enumerate((c, 1 - c)):
            block = wd.at[rows_of(2 * across + peer_c, ffw), :]
            remote(block, relay.at[n], relay_s, relay_r, (s, 2 * after_y + c))

    def relay_wd():
        arrived(relay, relay_r)
        for n, peer_c in enumerate((c, 1 - c)):
            remote(relay.at[n], wdt.at[2 * before_y + c], wdt_s, wdt_r, (s, 2 * after_y + peer_c))

    @pl.when(s < experts - 1)
    def _():
        remote(tail, halo, halo_s, halo_r, ((s + 1) % experts, j))

    give_wd(y, 1 - c)
    give_wd_at(1)

    @pl.when(s == 0)
    def _():
        halo[...] = jnp.zeros_like(halo)

    @pl.when(s > 0)
    def _():
        arrived(halo, halo_r)

    early = convolve(jnp.concatenate([halo[...], gated[:, :LANES]], axis=1).astype(F32))
    filtered = jnp.concatenate([early, later], axis=1)
    stats[j, 0:1, :] = jnp.sum(filtered, axis=0, keepdims=True)
    stats[j, 1:2, :] = jnp.sum(filtered * filtered, axis=0, keepdims=True)

    for k in far_first:
        remote(stats.at[j], stats.at[j], stat_s, stat_r, (s, lax.rem(j + k, tp)))
    for reach in range(2, ha - 1):
        give_wd_at(reach)
    arrived(stats.at[pl.ds(0, tp - 1)], stat_r)
    totals = jnp.sum(stats[...], axis=0)
    mean = totals[0:1] / channels
    var = totals[1:2] / channels - mean * mean
    normed = (filtered - mean) * lax.rsqrt(var + 1e-05) * tap[0:own_ch, taps : taps + 1]
    act[j] = (normed / (1.0 + jnp.exp(-normed))).astype(BF)

    def act_from(d):
        return act.at[2 * ((y - d + 2 * ny) % ny) + c]

    def send_act(d, reach):
        ref = act_from(d)
        remote(ref, ref, act_s, act_r.at[(d + reach) % ny], (s, 2 * ((y + reach + ny) % ny) + c))

    def share_act(d):
        ref = act_from(d)
        arrived(ref, act_r.at[d % ny])
        remote(ref, ref, act_s, act_sib, (s, sib))

    for reach in range(halfway, 0, -1):
        send_act(0, reach)
        send_act(0, -reach)
    remote(act.at[j], act.at[j], act_s, act_sib, (s, sib))
    for side in (1, -1):
        share_act(side * halfway)
        for reach in range(1, halfway):
            send_act(side * halfway, side * reach)

        @pl.when(lean == side)
        def _():
            send_act(side * halfway, side * halfway)

    give_wd_across()
    if ha > 2:
        give_wd_at(ha - 1)
    for d in range(1, halfway):
        share_act(d)
        share_act(-d)
    for d in range(halfway + 1, ha):
        share_act(d)
        share_act(-d)
    share_act(ha)
    arrived(act.at[pl.ds(0, ny)], act_sib)
    loads[3].wait()
    loads[4].wait()
    projected = lax.dot_general(
        act[...].reshape(tp * own_ch, tokens),
        proj[...],
        (((0,), (0,)), ((), ())),
        preferred_element_type=F32,
    )
    mixed[...] = (resid[...].astype(F32) + projected).astype(BF)

    outg[...] = dot(pick[...], mixed[...]).astype(BF)
    rows[z, c, y, rows_of(x, cap), :] = outg[rows_of(s, cap), :]

    for i in range(nz):
        zt = lax.rem(z + (nz - i), nz)
        for dx in range(nx):
            if i + dx == 0:
                continue
            e = zt * nx + lax.rem(x + dx, nx)
            remote(
                outg.at[rows_of(e, cap), :],
                rows.at[z, c, y, rows_of(x, cap), :],
                dsend,
                drecv.at[z],
                (e, j),
            )

    relay_wd()
    above = 2 * lax.rem(y + 1, ny) + c
    below = 2 * lax.rem(y + (ny - 1), ny) + c

    def toward(odd, leg):
        return (s, above + (odd if leg == 0 else 1 - odd) * (below - above))

    def chip(step, k):
        return lax.rem(y + step * k + ny, ny)

    def push(q, i, origin_y, hop, leg, odd):
        ref = rows.at[q, c, origin_y]
        remote(ref, ref, rsend.at[i], rring.at[i, leg * ha + hop], toward(odd, leg))

    def tick(t, carry):
        def at(stage, body):
            i = t - stage

            @pl.when((i >= 0) & (i < nz))
            def _():
                body(i, lax.rem(z + i, nz), lax.rem(i, 2))

        def rows_open(i, q, odd):
            @pl.when(i == 0)
            def _():
                if nx > 1:
                    arrived(outg.at[pl.ds(0, (nx - 1) * cap), :], drecv.at[q])

            @pl.when(i > 0)
            def _():
                arrived(outg.at[pl.ds(0, nx * cap), :], drecv.at[q])

            push(q, i, y, 0, 0, odd)
            if hb > 0:
                push(q, i, y, 0, 1, odd)

        def rows_hop(h, i, q, odd):
            for leg, reach in ((0, ha), (1, hb)):
                if h > reach:
                    continue
                origin = chip((2 * odd - 1) * (1 - 2 * leg), h)
                arrived(rows.at[q, c, origin], rring.at[i, leg * ha + h - 1])
                if h < reach:
                    push(q, i, origin, h, leg, odd)
            if h == ha:
                remote(rows.at[q, c], rows.at[q, c], rsend.at[i], rsib.at[i], (s, sib))

        def expert(i, q, odd):
            @pl.when(i == 0)
            def _():
                loads[5].wait()
                loads[6].wait()
                arrived(wd.at[pl.ds(0, (tp - 1) * ffw), :], wdt_r)

            arrived(rows.at[q, 0], rsib.at[i])
            r = jnp.concatenate([rows[q, b % 2, b // 2] for b in range(tp)], axis=1)
            g = dot(r, wg[...])
            u = dot(r, wu[...])
            h = ((g / (1.0 + jnp.exp(-g))) * u).astype(BF)
            for b in range(ny):
                w = jnp.concatenate([wdt[2 * b + c], wdt[2 * b + 1 - c]], axis=1)
                part = dot(h, w)
                own[i, b] = part[:, :width]
                give[i, b] = part[:, width:].astype(BF)
            remote(give.at[i], take.at[i], sib_s.at[i], sib_r.at[i], (s, sib))

        def mine(i, b):
            return own[i, b] + take[i, b].astype(F32)

        def sum_hop(m, i, q, odd):
            if m == 1:
                arrived(take.at[i], sib_r.at[i])
            for leg, reach in ((0, ha), (1, hb)):
                if m > reach:
                    continue
                k = reach - m + 1
                n = leg * ha + m - 1
                total = mine(i, chip((1 - 2 * odd) * (1 - 2 * leg), k))
                if m > 1:
                    arrived(sumin.at[i, n - 1], sum_r.at[i, n - 1])
                    total = total + sumin[i, n - 1].astype(F32)
                sumout[i, n] = total.astype(BF)
                ref = sumout.at[i, n]
                remote(ref, sumin.at[i, n], sum_s.at[i], sum_r.at[i, n], toward(odd, leg))

        def finish(i, q, odd):
            total = mine(i, y)
            for n in ([ha - 1, ny - 2] if hb > 0 else [ha - 1]):
                arrived(sumin.at[i, n], sum_r.at[i, n])
                total = total + sumin[i, n].astype(F32)
            res[i] = total.astype(BF)
            for xt in range(nx):
                tgt = q * nx + xt

                @pl.when(tgt == s)
                def _():
                    ret[rows_of(s, cap), :] = res[i, pl.ds(xt * cap, cap), :]

                @pl.when(tgt != s)
                def _():
                    remote(
                        res.at[i, pl.ds(xt * cap, cap), :],
                        ret.at[rows_of(s, cap), :],
                        bsend,
                        brecv,
                        (tgt, j),
                    )

        last = 2 * ha + 2
        at(2 * last - 2, finish)
        for m in range(ha, 0, -1):
            at(last + 2 * (m - 1), functools.partial(sum_hop, m))
        for h in range(ha, 0, -1):
            at(2 * h, functools.partial(rows_hop, h))
        at(0, rows_open)
        at(last - 1, expert)
        return carry

    lax.fori_loop(0, nz + 4 * ha + 2, tick, 0)

    far = outg.at[pl.ds(0, (experts - 1) * cap), :]
    arrived(far, brecv)
    back = ret[...]
    routed = dot(pick0[...], back) * scales[:, 2:3] + dot(pick1[...], back) * scales[:, 3:4]
    out_ref[...] = (mixed[...].astype(F32) + routed).astype(BF)

    @pl.when(s < experts - 1)
    def _():
        arrived(halo, halo_s)

    arrived(wd.at[pl.ds(0, (tp - 1) * ffw), :], wdt_s)
    arrived(relay, relay_s)
    arrived(stats.at[pl.ds(0, tp - 1)], stat_s)
    arrived(act.at[pl.ds(0, 2 * ny - 1)], act_s)
    arrived(far, dsend)
    arrived(far, bsend)

    def drain(i, carry):
        arrived(rows.at[0, 0], rsend.at[i])
        arrived(rows.at[0, 0, pl.ds(0, ny - 1)], rsend.at[i])
        arrived(give.at[0], sib_s.at[i])
        arrived(sumout.at[0], sum_s.at[i])
        return carry

    lax.fori_loop(0, nz, drain, 0)


def per_device(
    glu_value,
    glu_gate,
    conv_taps,
    norm_gain,
    out_proj,
    resid,
    expert_ids,
    route_logits,
    group_prob,
    w_gate,
    w_up,
    w_down,
):
    sp, tp = lax.axis_size("sp"), lax.axis_size("tp")
    nx = 4 if sp % 8 == 0 else 1
    nz, ny = sp // nx, tp // 2
    tokens, width = resid.shape
    cap = 4 * tokens // sp
    depth, ffw = w_gate.shape[1:]
    own_ch, taps = conv_taps.shape
    chunk = nx * cap
    dma = pltpu.SemaphoreType.DMA
    vmem = pl.BlockSpec(memory_space=pltpu.VMEM)
    hbm = pl.BlockSpec(memory_space=pl.ANY)
    dims = (nx, nz, ny, cap, taps, own_ch * tp)
    return pl.pallas_call(
        functools.partial(layer_kernel, dims),
        out_shape=jax.ShapeDtypeStruct((tokens, width), BF),
        in_specs=[hbm, hbm, vmem, vmem, hbm, hbm, vmem, vmem, vmem, hbm, hbm, hbm],
        out_specs=vmem,
        scratch_shapes=[
            pltpu.VMEM(glu_value.shape, BF),
            pltpu.VMEM(glu_gate.shape, BF),
            pltpu.VMEM(out_proj.shape, BF),
            pltpu.VMEM(resid.shape, BF),
            pltpu.VMEM((depth, ffw), BF),
            pltpu.VMEM((depth, ffw), BF),
            pltpu.VMEM(w_down.shape[1:], BF),
            pltpu.VMEM((tp, ffw, width), BF),
            pltpu.VMEM((32, LANES), F32),
            pltpu.VMEM((own_ch, LANES), BF),
            pltpu.VMEM((own_ch, LANES), BF),
            pltpu.VMEM((tp, 2, tokens), F32),
            pltpu.VMEM((tp, own_ch, tokens), BF),
            pltpu.VMEM((sp * cap, tokens), BF),
            pltpu.VMEM((tokens, sp * cap), BF),
            pltpu.VMEM((tokens, sp * cap), BF),
            pltpu.VMEM((tokens, 8), F32),
            pltpu.VMEM((tokens, width), BF),
            pltpu.VMEM((sp * cap, width), BF),
            pltpu.VMEM((nz, 2, ny, chunk, width), BF),
            pltpu.VMEM((nz, ny, chunk, width), F32),
            pltpu.VMEM((nz, ny, chunk, width), BF),
            pltpu.VMEM((nz, ny, chunk, width), BF),
            pltpu.VMEM((nz, ny - 1, chunk, width), BF),
            pltpu.VMEM((nz, ny - 1, chunk, width), BF),
            pltpu.VMEM((nz, chunk, width), BF),
            pltpu.VMEM((sp * cap, width), BF),
            dma((7,)),
            dma(()),
            dma(()),
            dma(()),
            dma(()),
            dma(()),
            dma((ny,)),
            dma(()),
            pltpu.VMEM((2, ffw, width), BF),
            dma(()),
            dma(()),
            dma(()),
            dma(()),
            dma(()),
            dma((nz,)),
            dma((nz, ny - 1)),
            dma((nz,)),
            dma((nz,)),
            dma((nz,)),
            dma((nz,)),
            dma((nz,)),
            dma((nz, ny - 1)),
            dma(()),
            dma(()),
        ],
        compiler_params=pltpu.CompilerParams(
            collective_id=0, has_side_effects=True, vmem_limit_bytes=63 * 1024 * 1024
        ),
    )(
        glu_value,
        glu_gate,
        conv_taps.T,
        norm_gain[None, :],
        out_proj,
        resid,
        expert_ids.T,
        route_logits.T,
        group_prob[None, :],
        w_gate,
        w_up,
        w_down,
    )


def solution(mesh):
    return jax.shard_map(
        per_device,
        mesh=mesh,
        in_specs=(
            P("tp", "sp"),
            P("tp", "sp"),
            P("tp", None),
            P("tp"),
            P(None, "tp"),
            P("sp", "tp"),
            P("sp", None),
            P("sp", None),
            P("sp"),
            P("sp", None, "tp"),
            P("sp", None, "tp"),
            P("sp", None, "tp"),
        ),
        out_specs=P("sp", "tp"),
        check_vma=False,
    )
```
